32 devices in a mesh: ep: 8 (over z, core), tp: 4 (over y, x).
Axes of the slice: x: 2, y: 2, z: 4, core: 2. Of those that a mesh axis runs over, the one named last changes fastest.
Arguments:
- query_maps: bfloat16 [1024, 16, 128], P('ep', 'tp'), may hold values from -6 to 6
- key_maps: bfloat16 [1024, 16, 128], P('ep', 'tp'), may hold values from -6 to 6
- value_rows: bfloat16 [1024, 16, 128], P('ep', 'tp'), may hold values from -6 to 6
- head_lambda: float32 [16], P('tp'), may hold values from 0.3 to 0.8
- head_gain: float32 [128], replicated, may hold values from 0.1 to 1.9
- out_weight: bfloat16 [2048, 2048], P('tp'), may hold values from -0.125 to 0.125
- token_rows: bfloat16 [1024, 2048], P('ep'), may hold values from -36 to 36
- norm_gain: float32 [2048], replicated, may hold values from 0.1 to 1.9
- expert_ids: int32 [1024, 4], P('ep'), may hold values from 0 to 7, all different within a row; in each aligned block of 128 rows (0 to 127, 128 to 255, ...) at most 80 rows name the same one
- route_weights: float32 [1024, 4], P('ep'), may hold values from 0.1 to 0.5
- gate_weight: bfloat16 [8, 2048, 4096], P('ep', None, 'tp'), may hold values from -0.82864076 to 0.82864076
- up_weight: bfloat16 [8, 2048, 4096], P('ep', None, 'tp'), may hold values from -0.82864076 to 0.82864076
- down_weight: bfloat16 [8, 4096, 2048], P('ep', 'tp'), may hold values from -0.03125 to 0.03125
Outputs:
- mixed_rows: bfloat16 [1024, 2048], P(('ep', 'tp'))
- mixed_experts: bfloat16 [1024, 2048], P('ep', 'tp')
The draws below stay inside these ranges and needn't reach their ends.
Inputs may be any that keep to these rules, and one draw needn't show every extreme that they name: `expert_ids`: each row names 4 different experts. Among the rows of one index of ep no expert is named more than 80 times, and in every draw some expert is named exactly 80 times there.
All inputs are finite; a program needn't handle non-finite values.
Results may differ from the reference program's by a relative error of at most 0.015.
Values may be sent and summed in bfloat16 or wider, within the bound.
A program may use at most 64 MiB of HBM per device.

```python
import math
import jax
import jax.numpy as jnp
import numpy as np
from jax import lax

D = 2048
HEADS = 16
HEAD_DIM = 64
FF = 4096
TOPK = 4
TOKB_DEV = 128
EXPERTS = 8
TOKA = 1024
TOKB = 1024
CAP = 80
N_EP = 8
N_TP = 4


def score_pair(key):
    parts = jax.random.split(jax.random.fold_in(key, 11), 3)
    full_shape = (TOKA, HEADS, 2 * HEAD_DIM)
    query_vals = jnp.clip(1.3 * jax.random.normal(parts[1], full_shape, jnp.float32), -6.0, 6.0)
    key_vals = jnp.clip(1.3 * jax.random.normal(parts[2], full_shape, jnp.float32), -6.0, 6.0)
    return (query_vals.astype(jnp.bfloat16), key_vals.astype(jnp.bfloat16))


def draw_query_maps(key, part):
    return score_pair(key)[0]


def draw_key_maps(key, part):
    return score_pair(key)[1]


def draw_token_rows(key, part):
    parts = jax.random.split(jax.random.fold_in(key, 23), 3)
    row_scales = jnp.exp(jax.random.uniform(parts[0], (TOKB, 1), jnp.float32, math.log(0.3), math.log(3.0)))
    values = jnp.clip(jax.random.normal(parts[1], (TOKB, D), jnp.float32), -4.0, 4.0)
    col_scales = jnp.exp(jax.random.uniform(parts[2], (1, D), jnp.float32, math.log(0.3), math.log(3.0)))
    return (values * row_scales * col_scales).astype(jnp.bfloat16)


def expert_matrix(key, salt_value):
    parts = jax.random.split(jax.random.fold_in(key, salt_value), 1)
    full_shape = (EXPERTS, D, FF)
    values = jnp.clip(jax.random.normal(parts[0], full_shape, jnp.float32), -6.0, 6.0) * (2.5 * D ** (-0.5))
    return values.astype(jnp.bfloat16)


def draw_gate_weight(key, part):
    return expert_matrix(key, 31)


def draw_up_weight(key, part):
    return expert_matrix(key, 37)


def block_levels(own_key, shape, shards, smallest, high):
    def one(axis_at, shards_of):
        heights = jax.random.uniform(jax.random.fold_in(jax.random.fold_in(own_key, 6), axis_at), (shards_of,), jnp.float32, smallest / len(shards), high / len(shards))
        return jnp.repeat(jnp.exp(heights), shape[axis_at] // shards_of).reshape((-1,) + (1,) * (len(shape) - axis_at - 1))

    gain = one(*shards[0])
    for cut in shards[1:]:
        gain = gain * one(*cut)
    return gain


def assign_block(stream_key, own, number, rows, number_of, top, limit, lean):
    ranking = jax.random.permutation(stream_key, number_of)
    crowded, common = load_shares(number_of, rows * top, limit, lean, True), load_shares(number_of, rows * top, limit, lean, False)
    places = jnp.arange(number_of)

    def named(sizes, rotation):
        used = int((sizes > 0).sum())
        fixed = max(1, used // 4)
        moved = fixed + (places - fixed + rotation * (used - fixed)) % max(1, number_of - fixed)
        return jnp.zeros((number_of,), jnp.int32).at[ranking[jnp.where(places < fixed, places, moved)]].set(jnp.asarray(sizes, jnp.int32))

    sizes = jnp.where(number % 4 == 0, named(crowded, number // 4), named(common, number - number // 4 - 1))
    mixed = jax.random.permutation(jax.random.fold_in(own, 3), number_of)
    giver, receiver = mixed[0:number_of // 2 * 2:2], mixed[1:number_of // 2 * 2:2]
    margin = jnp.minimum(sizes[giver] - 1, limit - sizes[receiver]) // 2
    margin = jnp.where((giver == ranking[0]) | (receiver == ranking[0]) | (sizes[receiver] == 0), 0, jnp.maximum(margin, 0))
    moved = jax.random.randint(jax.random.fold_in(own, 4), (number_of // 2,), 0, 1 << 20) % (margin + 1)
    sizes = sizes.at[giver].add(-moved).at[receiver].add(moved)
    members = jnp.searchsorted(jnp.cumsum(sizes), jnp.arange(rows * top), side="right").astype(jnp.int32)
    table = members.reshape(top, rows).T
    table = table[jax.random.permutation(jax.random.fold_in(own, 1), rows)]
    rotation = jax.random.randint(jax.random.fold_in(own, 2), (rows, 1), 0, top)
    return jnp.take_along_axis(table, (jnp.arange(top)[None, :] + rotation) % top, axis=1)


def load_shares(number_of, total, limit, lean, full):
    loads = [(1 << 20) // math.isqrt(rank ** lean) + 1 for rank in range(1, number_of + 1)]
    largest = limit if full else min(limit, max(-(-total // number_of), total * loads[0] // sum(loads)))
    least = 1 if total - largest >= number_of - 1 else 0
    given, spare = [largest] + [least] * (number_of - 1), total - largest - least * (number_of - 1)
    while spare > 0:
        movable = [i for i in range(1, number_of) if given[i] < largest] or [i for i in range(1, number_of) if given[i] < limit]
        mass, left = sum([loads[i] for i in movable]), spare
        for i in movable:
            extra = min(limit - given[i], max(1, left * loads[i] // mass), spare)
            given[i] = given[i] + extra
            spare = spare - extra
    return np.array(given)


def scatter_about(stream_key, dims, width, most, cuts=(), kind=jnp.bfloat16):
    entries = width * jax.random.normal(stream_key, dims, jnp.float32)
    if cuts:
        entries = entries * block_levels(stream_key, dims, cuts, -0.22, 0.18)
    return jnp.clip(entries, -most, most).astype(kind)


def setup_inputs(seed: int = 0) -> dict:
    keys = jax.random.split(jax.random.key(seed), 14)
    query_maps = draw_query_maps(jax.random.fold_in(keys[13], 71), 0)
    key_maps = draw_key_maps(jax.random.fold_in(keys[13], 71), 0)
    value_rows = scatter_about(keys[2], (TOKA, HEADS, 2 * HEAD_DIM), 1.0, 6.0, ((0, 8), (1, 4)))
    head_lambda = jnp.clip(0.3 + 0.5 * jax.random.uniform(keys[3], (HEADS,), jnp.float32) ** block_levels(keys[3], (HEADS,), ((0, 4),), -0.2, 0.2), 0.3, 0.8)
    head_gain = jnp.clip(1.0 + 0.18 * jax.random.normal(keys[4], (2 * HEAD_DIM,), jnp.float32), 0.1, 1.9)
    out_weight = scatter_about(keys[5], (HEADS * 2 * HEAD_DIM, D), (HEADS * 2 * HEAD_DIM) ** -0.5, 0.125, ((0, 4),))
    token_rows = draw_token_rows(jax.random.fold_in(keys[13], 71), 0)
    norm_gain = jnp.clip(1.0 + 0.18 * jax.random.normal(keys[7], (D,), jnp.float32), 0.1, 1.9)
    expert_ids_keys = jax.random.split(jax.random.fold_in(keys[8], 1), TOKB // TOKB_DEV)
    expert_ids_turns = jax.random.permutation(jax.random.fold_in(keys[8], 3), TOKB // TOKB_DEV)
    expert_ids = jax.vmap(lambda own, number: assign_block(jax.random.fold_in(keys[8], 2), own, number, TOKB_DEV, EXPERTS, TOPK, CAP, 1))(expert_ids_keys, expert_ids_turns).reshape((TOKB, TOPK))
    route_weights = jnp.clip(0.1 + 0.4 * jax.random.uniform(keys[9], (TOKB, TOPK), jnp.float32) ** block_levels(keys[9], (TOKB, TOPK), ((0, 8),), -0.2, 0.2), 0.1, 0.5)
    gate_weight = draw_gate_weight(jax.random.fold_in(keys[13], 71), 0)
    up_weight = draw_up_weight(jax.random.fold_in(keys[13], 71), 0)
    down_weight = scatter_about(keys[12], (EXPERTS, FF, D), (8 * FF) ** -0.5, 0.03125, ((0, 8), (1, 4)))
    return dict(query_maps=query_maps, key_maps=key_maps, value_rows=value_rows, head_lambda=head_lambda, head_gain=head_gain, out_weight=out_weight, token_rows=token_rows, norm_gain=norm_gain, expert_ids=expert_ids, route_weights=route_weights, gate_weight=gate_weight, up_weight=up_weight, down_weight=down_weight)


NORM_EPS = 1e-05
CLAMP_LIMIT = 7.0
GATE_SLOPE = 1.702

def rounded(values):
    return lax.optimization_barrier(values.astype(jnp.bfloat16)).astype(jnp.float32)

def mixer_half(query_maps, key_maps, value_rows, head_lambda, head_gain, out_weight):
    head_width = HEAD_DIM
    score_scale = head_width ** (-0.5)
    block_len = math.gcd(TOKA, 256)
    key_float = key_maps.astype(jnp.float32)
    value_float = value_rows.astype(jnp.float32)
    outputs = []
    for begin_at in range(0, TOKA, block_len):
        ending = begin_at + block_len
        query_float = query_maps[begin_at:ending].astype(jnp.float32)
        query_pos = begin_at + jnp.arange(block_len, dtype=jnp.int32)
        key_pos = jnp.arange(ending, dtype=jnp.int32)
        causal = key_pos[None, :] <= query_pos[:, None]
        results = []
        for map_index in range(2):
            col_low = map_index * head_width
            col_high = col_low + head_width
            scores = jnp.einsum('qhd,khd->hqk', query_float[:, :, col_low:col_high], key_float[:ending, :, col_low:col_high]) * score_scale
            scores = jnp.where(causal[None], scores, -jnp.inf)
            row_max = lax.optimization_barrier(jnp.max(scores, axis=-1, keepdims=True))
            exp_terms = jnp.exp(scores - row_max)
            denominator = lax.optimization_barrier(jnp.sum(exp_terms, axis=-1))
            weights = rounded(exp_terms)
            numerator = jnp.einsum('hqk,khd->qhd', weights, value_float[:ending])
            results.append(numerator / jnp.transpose(denominator)[:, :, None])
        attended = results[0] - head_lambda[None, :, None] * results[1]
        mean_sq = lax.optimization_barrier(jnp.mean(attended * attended, axis=-1, keepdims=True))
        normed = attended * lax.rsqrt(mean_sq + NORM_EPS) * head_gain
        outputs.append(normed.astype(jnp.bfloat16))
    head_rows = jnp.concatenate(outputs, axis=0).reshape(TOKA, HEADS * 2 * HEAD_DIM)
    group_width = HEADS * 2 * HEAD_DIM // N_TP
    summed = jnp.zeros((TOKA, D), jnp.float32)
    for group_index in range(N_TP):
        group_rows = head_rows[:, group_index * group_width:(group_index + 1) * group_width]
        group_weight = out_weight[group_index * group_width:(group_index + 1) * group_width]
        summed = summed + rounded(jnp.dot(group_rows, group_weight, preferred_element_type=jnp.float32))
    return summed.astype(jnp.bfloat16)

def expert_half(token_rows, norm_gain, expert_ids, route_weights, gate_weight, up_weight, down_weight):
    rows_float = token_rows.astype(jnp.float32)
    mean_sq = lax.optimization_barrier(jnp.mean(rows_float * rows_float, axis=-1, keepdims=True))
    normed = (rows_float * lax.rsqrt(mean_sq + NORM_EPS) * norm_gain).astype(jnp.bfloat16)
    flat_ids = expert_ids.reshape(N_EP, TOKB_DEV * TOPK)
    onehot = (flat_ids[:, :, None] == jnp.arange(EXPERTS, dtype=jnp.int32)[None, None, :]).astype(jnp.int32)
    rank_before = jnp.cumsum(onehot, axis=1) - onehot
    slot_of = lax.optimization_barrier(jnp.sum(rank_before * onehot, axis=2)).astype(jnp.int32)
    sources = jnp.arange(N_EP, dtype=jnp.int32)[:, None]
    token_of = sources * TOKB_DEV + jnp.arange(TOKB_DEV * TOPK, dtype=jnp.int32)[None, :] // TOPK
    row_index = sources * CAP + slot_of
    slot_table = jnp.full((EXPERTS, N_EP * CAP), TOKB, jnp.int32).at[flat_ids, row_index].set(token_of)
    padded = jnp.concatenate([normed, jnp.zeros((1, D), jnp.bfloat16)], axis=0)

    def one_expert(inputs):
        row_ids, gate_matrix, up_matrix, down_matrix = inputs
        chosen = padded[row_ids]
        gate_pre = jnp.dot(chosen, gate_matrix, preferred_element_type=jnp.float32)
        up_pre = jnp.dot(chosen, up_matrix, preferred_element_type=jnp.float32)
        gated = jnp.minimum(gate_pre, CLAMP_LIMIT)
        clipped = jnp.clip(up_pre, -CLAMP_LIMIT, CLAMP_LIMIT)
        active = rounded((clipped + 1.0) * gated * jax.nn.sigmoid(GATE_SLOPE * gated))
        grouped = active.reshape(N_EP * CAP, N_TP, FF // N_TP)
        down_grouped = down_matrix.astype(jnp.float32).reshape(N_TP, FF // N_TP, D)
        terms = jnp.einsum('rgf,gfd->rgd', grouped, down_grouped)
        return lax.optimization_barrier(jnp.sum(rounded(terms), axis=1)).astype(jnp.bfloat16)
    expert_out = lax.map(one_expert, (slot_table, gate_weight, up_weight, down_weight))
    picked = expert_out[flat_ids.reshape(-1), row_index.reshape(-1)].astype(jnp.float32)
    combined = lax.optimization_barrier(jnp.sum(picked.reshape(TOKB, TOPK, D) * route_weights[:, :, None], axis=1))
    return combined.astype(jnp.bfloat16)

def reference(query_maps, key_maps, value_rows, head_lambda, head_gain, out_weight, token_rows, norm_gain, expert_ids, route_weights, gate_weight, up_weight, down_weight):
    mixed_rows = mixer_half(query_maps, key_maps, value_rows, head_lambda, head_gain, out_weight)
    mixed_experts = expert_half(token_rows, norm_gain, expert_ids, route_weights, gate_weight, up_weight, down_weight)
    return (mixed_rows, mixed_experts)
```

```python
import functools

import jax
import jax.numpy as jnp
from jax import lax
from jax.experimental import pallas as pl
from jax.experimental.pallas import tpu as pltpu
from jax.sharding import PartitionSpec as P

NORM_EPS = 1e-05
CLAMP_LIMIT = 7.0
GATE_SLOPE = 1.702
CORES = 2
F32 = jnp.float32
BF16 = jnp.bfloat16


def remote(src, dst, send_sem, recv_sem, ep, tp):
    return pltpu.make_async_remote_copy(
        src_ref=src,
        dst_ref=dst,
        send_sem=send_sem,
        recv_sem=recv_sem,
        device_id={"ep": ep, "tp": tp},
        device_id_type=pl.DeviceIdType.MESH,
    )


def kernel(
    n_ep,
    n_tp,
    route_count,
    head_width,
    by_head,
    q_ref,
    k_ref,
    v_ref,
    lam_ref,
    gain_ref,
    rows_ref,
    norm_gain_ref,
    ids_ref,
    route_ref,
    ow_hbm,
    wg_hbm,
    wu_hbm,
    wd_hbm,
    out_rows_ref,
    out_exp_ref,
    ow,
    wg,
    wu,
    wd,
    xb,
    meta,
    own,
    kvb,
    hsend,
    hrecv,
    split,
    act,
    cbuf,
    pbuf,
    rbuf,
    ubuf,
    vbuf,
    prod,
    abuf,
    xs_s,
    xs_r,
    ms_s,
    ms_r,
    ks_s,
    ks_r,
    t_s,
    t_r,
    h_s,
    h_r,
    d_s,
    d_r,
    md_s,
    md_r,
    kd_s,
    kd_r,
    p_s,
    p_r,
    r_s,
    r_r,
    v_s,
    v_r,
    e_s,
    e_r,
    a_s,
    a_r,
    w_sem,
):
    nz = n_ep // CORES
    ep = lax.axis_index("ep")
    tp = lax.axis_index("tp")
    z = ep // CORES
    core = ep % CORES
    partner = z * CORES + (1 - core)
    tokens, model = rows_ref.shape
    quarter = model // n_tp
    hidden = wg.shape[1]
    width = 2 * head_width
    heads = q_ref.shape[0] // tokens

    weight_copies = [
        pltpu.make_async_copy(src, dst, w_sem.at[i])
        for i, (src, dst) in enumerate([(wg_hbm, wg), (wu_hbm, wu), (wd_hbm, wd), (ow_hbm, ow)])
    ]
    for copy in weight_copies:
        copy.start()

    barrier = pltpu.get_barrier_semaphore()

    def greet(e, t):
        pl.semaphore_signal(
            barrier, inc=1, device_id={"ep": e, "tp": t}, device_id_type=pl.DeviceIdType.MESH
        )

    greet(partner, tp)
    for off in range(1, nz):
        greet(((z + off) % nz) * CORES + core, tp)
    for off in range(1, n_tp):
        greet(ep, (tp + off) % n_tp)

    rows = rows_ref[...].astype(F32)
    mean_sq = jnp.mean(rows * rows, axis=-1, keepdims=True)
    normed = (rows * lax.rsqrt(mean_sq + NORM_EPS) * norm_gain_ref[...]).astype(BF16)
    for j in range(n_tp):
        xb[j, ep] = normed[:, j * quarter : (j + 1) * quarter]
    meta[ep, :route_count] = ids_ref[...].astype(F32)
    meta[ep, route_count : 2 * route_count] = route_ref[...]

    pl.semaphore_wait(barrier, 1 + (nz - 1) + (n_tp - 1))

    near = jnp.minimum(z, nz - 1 - z)
    far_sign = jnp.where(z < nz - 1 - z, 1, -1)

    def origin(i):
        alternate = ((i + 1) // 2) * ((i % 2) * 2 - 1)
        return z + jnp.where(i <= 2 * near, alternate, far_sign * (i - near))

    def line_copy(buf, send, recv, zo, way):
        block = buf.at[zo * CORES + core]
        return remote(
            block,
            block,
            send.at[way, zo],
            recv.at[zo],
            (z + (1 if way == 0 else -1)) * CORES + core,
            tp,
        )

    x_own = xb.at[tp]

    def each_line(buf, send, recv, zo, act_on):
        @pl.when((zo <= z) & (z < nz - 1))
        def _():
            act_on(line_copy(buf, send, recv, zo, 0))

        @pl.when((zo >= z) & (z > 0))
        def _():
            act_on(line_copy(buf, send, recv, zo, 1))

    square = n_tp == 4
    half = tokens // 2
    side = tp + 1 - 2 * (tp % 2)
    other = (tp + 2) % n_tp
    across = (side + 2) % n_tp
    halves = (pl.ds(0, half), pl.ds(half, half))
    targets = [side, other] if square else [(tp + off) % n_tp for off in range(1, n_tp)]

    def tp_copy(zo, n):
        block = xb.at[tp, zo * CORES + core]
        return remote(block, block, t_s.at[n, zo], t_r.at[tp, zo], ep, targets[n])

    def tp_arrival(zo, n):
        j = targets[n]
        block = xb.at[j, zo * CORES + core]
        return remote(block, block, t_s.at[n, zo], t_r.at[j, zo], ep, j)

    def pass_copy(zo, n):
        block = xb.at[other if n == 0 else side, zo * CORES + core, halves[n]]
        return remote(block, block, h_s.at[n, zo], h_r.at[n, zo], ep, targets[n])

    def pass_arrival(zo, n):
        block = xb.at[across, zo * CORES + core, halves[n]]
        return remote(block, block, h_s.at[n, zo], h_r.at[n, zo], ep, targets[n])

    def pair_copy(j, zo, mine=True):
        block = xb.at[j, zo * CORES + (core if mine else 1 - core)]
        return remote(block, block, d_s.at[j, zo], d_r.at[j, zo], partner, tp)

    def pair_block(buf, send, recv, zo, mine=True):
        block = buf.at[zo * CORES + (core if mine else 1 - core)]
        return remote(block, block, send.at[zo], recv.at[zo], partner, tp)

    start = lambda copy: copy.start()

    def take_x(zo):
        line_copy(x_own, xs_s, xs_r, zo, 0).wait_recv()
        each_line(x_own, xs_s, xs_r, zo, start)
        for n in range(len(targets)):
            tp_copy(zo, n).start()
        pair_copy(tp, zo).start()
        line_copy(meta, ms_s, ms_r, zo, 0).wait_recv()
        each_line(meta, ms_s, ms_r, zo, start)
        pair_block(meta, md_s, md_r, zo).start()

    def take_round(r):
        @pl.when(z + r < nz)
        def _():
            take_x(z + r)

        @pl.when(z - r >= 0)
        def _():
            take_x(z - r)

    def take_tp(zo):
        for n in range(len(targets)):
            tp_arrival(zo, n).wait_recv()
        if square:
            for n in range(2):
                pass_copy(zo, n).start()
        for j in targets:
            pair_copy(j, zo).start()

    def take_pass(zo):
        if square:
            for n in range(2):
                pass_arrival(zo, n).wait_recv()
            pair_copy(across, zo).start()

    def take_pair(zo):
        for j in range(n_tp):
            pair_copy(j, zo, False).wait_recv()
        pair_block(meta, md_s, md_r, zo, False).wait_recv()

    def spread_kv(zo):
        each_line(kvb, ks_s, ks_r, zo, start)
        pair_block(kvb, kd_s, kd_r, zo).start()

    def take_kv(zo):
        line_copy(kvb, ks_s, ks_r, zo, 0).wait_recv()
        spread_kv(zo)

    def head_copy(zo):
        return remote(
            own.at[zo], kvb.at[ep], ks_s.at[0, zo], ks_r.at[z], zo * CORES + core, tp
        )

    def head_arrival(zo):
        block = kvb.at[zo * CORES + core]
        return remote(block, block, ks_s.at[0, zo], ks_r.at[zo], zo * CORES + core, tp)

    def head_pair(zo, mine=True):
        block = kvb.at[zo * CORES + (core if mine else 1 - core), pl.ds(1, 2)]
        return remote(block, block, kd_s.at[zo], kd_r.at[zo], partner, tp)

    def back_copy(zo):
        return remote(
            hsend.at[zo], hrecv.at[z], e_s.at[zo], e_r.at[z], zo * CORES + core, tp
        )

    def back_arrival(zo):
        return remote(
            hsend.at[zo], hrecv.at[zo], e_s.at[zo], e_r.at[zo], zo * CORES + core, tp
        )

    order = [across, side, other, tp] if square else [(tp + off) % n_tp for off in range(1, n_tp + 1)]

    def half_copy(zo, j):
        return remote(
            cbuf.at[zo, 1 - core, j], pbuf.at[zo, j], p_s.at[j, zo], p_r.at[j, zo], partner, tp
        )

    def term_parts():
        everything = pl.ds(0, tokens)
        if square:
            return [
                (side, halves[0], side, side),
                (across, halves[0], side, across),
                (other, halves[1], other, other),
                (across, halves[1], other, across),
                (other, halves[0], other, side),
                (side, halves[1], side, other),
            ]
        return [(j, everything, j, tp) for j in targets]

    def term_copy(zo, n):
        j, rows_of, device, slot = term_parts()[n]
        return remote(
            cbuf.at[zo, core, j, rows_of],
            rbuf.at[zo, slot, rows_of],
            r_s.at[n, zo],
            r_r.at[n, zo] if square else r_r.at[tp, zo],
            ep,
            device,
        )

    def term_arrival(zo, n):
        if square:
            slot = [tp, other, tp, side, across, across][n]
            rows_of = term_parts()[n][1]
            device = term_parts()[n][2]
            sem = r_r.at[n, zo]
        else:
            slot = device = targets[n]
            rows_of = pl.ds(0, tokens)
            sem = r_r.at[slot, zo]
        return remote(
            cbuf.at[zo, core, device, rows_of],
            rbuf.at[zo, slot, rows_of],
            r_s.at[n, zo],
            sem,
            ep,
            device,
        )

    def finish(zo):
        sends = {0: (1, 3), 1: (0,), 2: (2,)} if square else {i: (i,) for i in range(n_tp - 1)}
        for i, j in enumerate(order):
            half_copy(zo, j).wait_recv()
            cbuf[zo, core, j] = (
                cbuf[zo, core, j].astype(F32) + pbuf[zo, j].astype(F32)
            ).astype(BF16)
            for n in sends.get(i, ()):
                term_copy(zo, n).start()

    def middle(zo):
        if square:
            for n, arrived, j in ((4, 1, other), (5, 3, side)):
                term_arrival(zo, arrived).wait_recv()
                rows_of = halves[n - 4]
                cbuf[zo, core, j, rows_of] = (
                    cbuf[zo, core, j, rows_of].astype(F32) + rbuf[zo, j, rows_of].astype(F32)
                ).astype(BF16)
                term_copy(zo, n).start()

    def home_copy(zo):
        return remote(
            ubuf.at[zo], vbuf.at[z], v_s.at[zo], v_r.at[z], zo * CORES + core, tp
        )

    def home_arrival(zo):
        return remote(
            ubuf.at[zo], vbuf.at[zo], v_s.at[zo], v_r.at[zo], zo * CORES + core, tp
        )

    def reduce(zo):
        total = cbuf[zo, core, tp].astype(F32)
        if square:
            for n in (0, 2, 4, 5):
                term_arrival(zo, n).wait_recv()
            total = total + rbuf[zo, tp].astype(F32) + rbuf[zo, across].astype(F32)
        else:
            for n, j in enumerate(targets):
                term_arrival(zo, n).wait_recv()
                total = total + rbuf[zo, j].astype(F32)
        ubuf[zo] = total.astype(BF16)

        @pl.when(zo != z)
        def _():
            home_copy(zo).start()

    tile = min(256, hidden)
    tiles = hidden // tile

    def hidden_tile(zo, f):
        pair = pl.ds(zo * CORES, CORES)
        cols = pl.ds(f * tile, tile)
        gate = jnp.zeros((CORES * tokens, tile), F32)
        up = jnp.zeros((CORES * tokens, tile), F32)
        for j in range(n_tp):
            chunk = xb[j, pair].reshape(CORES * tokens, quarter)
            depth = pl.ds(j * quarter, quarter)
            gate = gate + jnp.dot(chunk, wg[depth, cols], preferred_element_type=F32)
            up = up + jnp.dot(chunk, wu[depth, cols], preferred_element_type=F32)
        gated = jnp.minimum(gate, CLAMP_LIMIT)
        clipped = jnp.clip(up, -CLAMP_LIMIT, CLAMP_LIMIT)
        act[:, cols] = (
            (clipped + 1.0) * gated * jax.nn.sigmoid(GATE_SLOPE * gated)
        ).astype(BF16)

    eye = lax.broadcasted_iota(jnp.int32, (tokens, tokens), 0) == lax.broadcasted_iota(
        jnp.int32, (tokens, tokens), 1
    )

    def route_scale(zo):
        columns = []
        for c in range(CORES):
            info = meta[zo * CORES + c]
            named = info[:route_count] == ep.astype(F32)
            weights = jnp.where(named, info[route_count : 2 * route_count], 0.0)
            line = jnp.sum(weights, axis=0, keepdims=True)
            columns.append(jnp.sum(jnp.where(eye, line, 0.0), axis=1, keepdims=True))
        return jnp.concatenate(columns, axis=0)

    def model_tile(zo, j, scale):
        cols = pl.ds(pl.multiple_of(j * quarter, quarter), quarter)
        value = jnp.dot(act[...], wd[:, cols], preferred_element_type=F32) * scale
        value = value.astype(BF16)
        for c in range(CORES):
            cbuf[zo, c, j] = value[c * tokens : (c + 1) * tokens]
        half_copy(zo, j).start()

    each_line(x_own, xs_s, xs_r, z, start)
    for j in range(n_tp):
        pair_copy(j, z).start()
    each_line(meta, ms_s, ms_r, z, start)
    pair_block(meta, md_s, md_r, z).start()

    for part, ref in enumerate((q_ref, k_ref, v_ref)):
        split[...] = ref[...].astype(F32)
        for h in range(heads):
            own[h, part] = split[pl.ds(h, tokens, stride=heads), :].astype(BF16)
    if by_head:
        kvb[ep] = own[z]
        head_pair(z).start()
    else:
        for h in range(heads):
            for part in range(2):
                at = (part * heads + h) * width
                kvb[ep, :, at : at + width] = own[h, 1 + part]

    def step(i, carry):
        zo = origin(i)
        take_pair(zo)

        @pl.when(i == 0)
        def _():
            for copy in weight_copies[:2]:
                copy.wait()

        for f in range(tiles):
            hidden_tile(zo, f)
            if f == min(1, tiles - 1):

                @pl.when(i == 0)
                def _():
                    take_round(1)

                @pl.when(i > 1)
                def _():
                    middle(origin(i - 2))

                @pl.when(i > 0)
                def _():
                    finish(origin(i - 1))

        @pl.when((i > 0) & (i + 1 < nz))
        def _():
            take_pass(origin(i + 1))

        @pl.when(i == 0)
        def _():
            weight_copies[2].wait()

        scale = route_scale(zo)
        for j in order:
            model_tile(zo, j, scale)

        @pl.when(i == 0)
        def _():
            take_round(2)
            if by_head:
                for off in range(1, nz):
                    head_copy((z + off) % nz).start()
            else:
                spread_kv(z)
            if nz > 1:
                take_tp(origin(1))
                take_pass(origin(1))

        if not by_head:

            @pl.when(i > 0)
            def _():
                take_kv(zo)

        take_round(i + 3)

        @pl.when(i + 2 < nz)
        def _():
            take_tp(origin(i + 2))

        @pl.when(i > 1)
        def _():
            reduce(origin(i - 2))

        return carry

    lax.fori_loop(0, nz, step, 0)

    if by_head:
        for off in range(1, nz):
            zs = (z + off) % nz
            head_arrival(zs).wait_recv()
            head_pair(zs).start()
    finish(origin(nz - 1))
    middle(origin(nz - 2))

    gain = gain_ref[...]
    lane = lax.broadcasted_iota(jnp.int32, (tokens, width), 1)

    def both_maps(query):
        nothing = jnp.zeros_like(query)
        return jnp.concatenate(
            [jnp.where(lane < head_width, query, nothing), jnp.where(lane < head_width, nothing, query)],
            axis=0,
        )

    def head_norm(value_sum, total, lam):
        mean = value_sum / total
        attended = mean[:tokens] - lam * mean[tokens:]
        mean_sq = jnp.mean(attended * attended, axis=-1, keepdims=True)
        return (attended * lax.rsqrt(mean_sq + NORM_EPS) * gain).astype(BF16)

    def position_block(n):
        at = n * CORES + core
        extent = (n + 1) * CORES * tokens
        keys = kvb[: (n + 1) * CORES, 1].reshape(extent, width)
        values = kvb[: (n + 1) * CORES, 2].reshape(extent, width)
        score = lax.dot_general(
            both_maps(kvb[at, 0]), keys, (((1,), (1,)), ((), ())), preferred_element_type=F32
        ) * (head_width**-0.5)
        row = lax.broadcasted_iota(jnp.int32, (2 * tokens, extent), 0) % tokens + at * tokens
        col = lax.broadcasted_iota(jnp.int32, (2 * tokens, extent), 1)
        score = jnp.where(col <= row, score, -1e30)
        terms = jnp.exp(score - jnp.max(score, axis=1, keepdims=True))
        total = jnp.sum(terms, axis=1, keepdims=True)
        value_sum = jnp.dot(terms.astype(BF16), values, preferred_element_type=F32)
        result = head_norm(value_sum, total, lam_ref[z])
        hsend[n] = result

        @pl.when(z != n)
        def _():
            back_copy(n).start()

    key_blocks = min(n_ep, 8)
    key_span = key_blocks * tokens

    def one_head(h, carry):
        both = both_maps(own[h, 0])
        row = lax.broadcasted_iota(jnp.int32, (2 * tokens, key_span), 0) % tokens + ep * tokens
        col = lax.broadcasted_iota(jnp.int32, (2 * tokens, key_span), 1)
        cols = pl.ds(pl.multiple_of(h * width, width), width)
        value_cols = pl.ds(pl.multiple_of((heads + h) * width, width), width)

        def span(s, state):
            top, total, value_sum = state
            blocks = pl.ds(s * key_blocks, key_blocks)
            keys = kvb[blocks, :, cols].reshape(key_span, width)
            values = kvb[blocks, :, value_cols].reshape(key_span, width)
            score = lax.dot_general(
                both, keys, (((1,), (1,)), ((), ())), preferred_element_type=F32
            ) * (head_width**-0.5)
            score = jnp.where(col + s * key_span <= row, score, -1e30)
            new_top = jnp.maximum(top, jnp.max(score, axis=1, keepdims=True))
            terms = jnp.exp(score - new_top)
            keep = jnp.exp(top - new_top)
            total = total * keep + jnp.sum(terms, axis=1, keepdims=True)
            value_sum = value_sum * keep + jnp.dot(
                terms.astype(BF16), values, preferred_element_type=F32
            )
            return new_top, total, value_sum

        state = (
            jnp.full((2 * tokens, 1), -1e30, F32),
            jnp.zeros((2 * tokens, 1), F32),
            jnp.zeros((2 * tokens, width), F32),
        )
        state = lax.fori_loop(0, n_ep // key_blocks, span, state)
        hsend[h] = head_norm(state[2], state[1], lam_ref[h])
        return carry

    if by_head:
        for n in range(nz):
            head_pair(n, False).wait_recv()
        for n in range(nz):
            position_block(n)
        hrecv[z] = hsend[z]
        reduce(origin(nz - 2))
        middle(origin(nz - 1))
        for off in range(1, nz):
            back_arrival((z + off) % nz).wait_recv()
        head_rows = jnp.concatenate([hrecv[h] for h in range(heads)], axis=1)
    else:

        def wait_kv(i, carry):
            pair_block(kvb, kd_s, kd_r, i, False).wait_recv()
            return carry

        lax.fori_loop(0, nz, wait_kv, 0)
        lax.fori_loop(0, heads, one_head, 0)
        reduce(origin(nz - 2))
        middle(origin(nz - 1))
        head_rows = jnp.concatenate([hsend[h] for h in range(heads)], axis=1)
    weight_copies[3].wait()
    out_rows = tokens // n_tp

    for n in range(n_tp):
        cols = pl.ds(n * quarter, quarter)
        value = jnp.dot(head_rows, ow[:, cols], preferred_element_type=F32).astype(BF16)
        for j in range(n_tp):
            prod[j, :, cols] = value[j * out_rows : (j + 1) * out_rows]

    def row_copy(off):
        j = (tp + off) % n_tp
        return remote(prod.at[j], abuf.at[tp], a_s.at[off], a_r.at[tp], ep, j)

    def row_arrival(off):
        j = (tp + off) % n_tp
        return remote(prod.at[j], abuf.at[j], a_s.at[off], a_r.at[j], ep, j)

    for off in range(1, n_tp):
        row_copy(off).start()
    reduce(origin(nz - 1))

    mixed = prod[tp].astype(F32)
    for off in range(1, n_tp):
        row_arrival(off).wait_recv()
        mixed = mixed + abuf[(tp + off) % n_tp].astype(F32)
    out_rows_ref[...] = mixed

    combined = ubuf[z].astype(F32)
    for off in range(1, nz):
        zs = (z + off) % nz
        home_arrival(zs).wait_recv()
        combined = combined + vbuf[zs].astype(F32)
    out_exp_ref[...] = combined

    left = lambda copy: copy.wait_send()

    def drain(zo, carry):
        each_line(x_own, xs_s, xs_r, zo, left)
        each_line(meta, ms_s, ms_r, zo, left)
        for n in range(len(term_parts())):
            term_copy(zo, n).wait_send()
        for j in range(n_tp):
            pair_copy(j, zo).wait_send()
            half_copy(zo, j).wait_send()
        pair_block(meta, md_s, md_r, zo).wait_send()
        if by_head:
            head_pair(zo).wait_send()
        else:
            each_line(kvb, ks_s, ks_r, zo, left)
            pair_block(kvb, kd_s, kd_r, zo).wait_send()

        @pl.when(zo != z)
        def _():
            home_copy(zo).wait_send()
            for n in range(len(targets)):
                tp_copy(zo, n).wait_send()
            if square:
                for n in range(2):
                    pass_copy(zo, n).wait_send()
            if by_head:
                head_copy(zo).wait_send()
                back_copy(zo).wait_send()

        return carry

    lax.fori_loop(0, nz, drain, 0)
    for off in range(1, n_tp):
        row_copy(off).wait_send()


def body(
    query_maps,
    key_maps,
    value_rows,
    head_lambda,
    head_gain,
    out_weight,
    token_rows,
    norm_gain,
    expert_ids,
    route_weights,
    gate_weight,
    up_weight,
    down_weight,
):
    n_ep, n_tp = lax.axis_size("ep"), lax.axis_size("tp")
    nz = n_ep // CORES
    tokens, heads, width = query_maps.shape
    model = token_rows.shape[1]
    quarter = model // n_tp
    hidden = gate_weight.shape[2]
    routes = expert_ids.shape[1]
    span = heads * width
    by_head = heads == nz
    flat = (tokens * heads, width)
    vmem = pl.BlockSpec(memory_space=pltpu.VMEM)
    smem = pl.BlockSpec(memory_space=pltpu.SMEM)
    hbm = pl.BlockSpec(memory_space=pltpu.HBM)
    dma = pltpu.SemaphoreType.DMA
    line = [dma((2, nz)), dma((nz,))]
    line_sem = [dma((2, nz)), dma((2, nz))]
    grid_sem = [dma((n_tp, nz)), dma((n_tp, nz))]
    pair = [dma((nz,)), dma((nz,))]
    mixed_rows, mixed_experts = pl.pallas_call(
        functools.partial(kernel, n_ep, n_tp, routes, width // 2, by_head),
        out_shape=(
            jax.ShapeDtypeStruct((tokens // n_tp, model), F32),
            jax.ShapeDtypeStruct((tokens, quarter), F32),
        ),
        in_specs=[vmem, vmem, vmem, smem, vmem, vmem, vmem, vmem, vmem, hbm, hbm, hbm, hbm],
        out_specs=(vmem, vmem),
        scratch_shapes=[
            pltpu.VMEM(out_weight.shape, BF16),
            pltpu.VMEM((model, hidden), BF16),
            pltpu.VMEM((model, hidden), BF16),
            pltpu.VMEM((hidden, model), BF16),
            pltpu.VMEM((n_tp, n_ep, tokens, quarter), BF16),
            pltpu.VMEM((n_ep, 2 * routes, tokens), F32),
            pltpu.VMEM((heads, 3, tokens, width), BF16),
            pltpu.VMEM((n_ep, 3, tokens, width) if by_head else (n_ep, tokens, 2 * span), BF16),
            pltpu.VMEM((heads, tokens, width), BF16),
            pltpu.VMEM((heads, tokens, width), BF16),
            pltpu.VMEM(flat, F32),
            pltpu.VMEM((CORES * tokens, hidden), BF16),
            pltpu.VMEM((nz, CORES, n_tp, tokens, quarter), BF16),
            pltpu.VMEM((nz, n_tp, tokens, quarter), BF16),
            pltpu.VMEM((nz, n_tp, tokens, quarter), BF16),
            pltpu.VMEM((nz, tokens, quarter), BF16),
            pltpu.VMEM((nz, tokens, quarter), BF16),
            pltpu.VMEM((n_tp, tokens // n_tp, model), BF16),
            pltpu.VMEM((n_tp, tokens // n_tp, model), BF16),
            *line,
            *line,
            *line,
            *grid_sem,
            *line_sem,
            *grid_sem,
            *pair,
            *pair,
            *grid_sem,
            dma((max(6, n_tp), nz)),
            dma((max(6, n_tp), nz)),
            *pair,
            *pair,
            dma((n_tp,)),
            dma((n_tp,)),
            dma((4,)),
        ],
        compiler_params=pltpu.CompilerParams(
            collective_id=0, has_side_effects=True, vmem_limit_bytes=67043328
        ),
        name="layer",
    )(
        query_maps.reshape(flat),
        key_maps.reshape(flat),
        value_rows.reshape(flat),
        head_lambda,
        head_gain.reshape(1, -1),
        token_rows,
        norm_gain.reshape(1, -1),
        expert_ids.T,
        route_weights.T,
        out_weight,
        gate_weight[0],
        up_weight[0],
        down_weight[0],
    )
    return mixed_rows.astype(BF16), mixed_experts.astype(BF16)


def solution(mesh):
    placed = (
        P("ep", "tp", None),
        P("ep", "tp", None),
        P("ep", "tp", None),
        P("tp"),
        P(),
        P("tp", None),
        P("ep", None),
        P(),
        P("ep", None),
        P("ep", None),
        P("ep", None, "tp"),
        P("ep", None, "tp"),
        P("ep", "tp", None),
    )
    return jax.shard_map(
        body,
        mesh=mesh,
        in_specs=placed,
        out_specs=(P(("ep", "tp"), None), P("ep", "tp")),
        check_vma=False,
    )
```

```python
import functools

import jax
import jax.numpy as jnp
from jax import lax
from jax.experimental import pallas as pl
from jax.experimental.pallas import tpu as pltpu
from jax.sharding import PartitionSpec as P

NORM_EPS = 1e-05
CLAMP_LIMIT = 7.0
GATE_SLOPE = 1.702
CORES = 2
F32 = jnp.float32
BF16 = jnp.bfloat16


def remote(src, dst, send_sem, recv_sem, ep, tp):
    return pltpu.make_async_remote_copy(
        src_ref=src,
        dst_ref=dst,
        send_sem=send_sem,
        recv_sem=recv_sem,
        device_id={"ep": ep, "tp": tp},
        device_id_type=pl.DeviceIdType.MESH,
    )


def kernel(
    n_ep,
    n_tp,
    route_count,
    head_width,
    by_head,
    q_hbm,
    k_hbm,
    v_hbm,
    lam_hbm,
    gain_hbm,
    rows_hbm,
    norm_gain_hbm,
    ids_hbm,
    route_hbm,
    ow_hbm,
    wg_hbm,
    wu_hbm,
    wd_hbm,
    out_rows_ref,
    out_exp_ref,
    q_ref,
    k_ref,
    v_ref,
    lam_ref,
    gain_ref,
    rows_ref,
    norm_gain_ref,
    ids_ref,
    route_ref,
    ow,
    wg,
    wu,
    wd,
    xb,
    meta,
    own,
    kvb,
    hsend,
    hrecv,
    split,
    act,
    cbuf,
    pbuf,
    rbuf,
    ubuf,
    vbuf,
    prod,
    abuf,
    xs_s,
    xs_r,
    ms_s,
    ms_r,
    ks_s,
    ks_r,
    t_s,
    t_r,
    h_s,
    h_r,
    d_s,
    d_r,
    md_s,
    md_r,
    kd_s,
    kd_r,
    p_s,
    p_r,
    r_s,
    r_r,
    v_s,
    v_r,
    e_s,
    e_r,
    a_s,
    a_r,
    i_sem,
    w_sem,
):
    nz = n_ep // CORES
    ep = lax.axis_index("ep")
    tp = lax.axis_index("tp")
    z = ep // CORES
    core = ep % CORES
    partner = z * CORES + (1 - core)
    tokens, model = rows_ref.shape
    quarter = model // n_tp
    hidden = wg.shape[1]
    width = 2 * head_width
    heads = q_ref.shape[0] // tokens

    barrier = pltpu.get_barrier_semaphore()

    def greet(e, t):
        pl.semaphore_signal(
            barrier, inc=1, device_id={"ep": e, "tp": t}, device_id_type=pl.DeviceIdType.MESH
        )

    greet(partner, tp)
    for off in range(1, nz):
        greet(((z + off) % nz) * CORES + core, tp)
    for off in range(1, n_tp):
        greet(ep, (tp + off) % n_tp)

    inputs = [
        (rows_hbm, rows_ref),
        (norm_gain_hbm, norm_gain_ref),
        (ids_hbm, ids_ref),
        (route_hbm, route_ref),
        (q_hbm, q_ref),
        (k_hbm, k_ref),
        (v_hbm, v_ref),
        (lam_hbm, lam_ref),
        (gain_hbm, gain_ref),
    ]
    input_copies = [
        pltpu.make_async_copy(src, dst, i_sem.at[i]) for i, (src, dst) in enumerate(inputs)
    ]
    weight_copies = [
        pltpu.make_async_copy(src, dst, w_sem.at[i])
        for i, (src, dst) in enumerate([(wg_hbm, wg), (wu_hbm, wu), (wd_hbm, wd), (ow_hbm, ow)])
    ]
    for copy in input_copies + weight_copies:
        copy.start()
    for copy in input_copies[:4]:
        copy.wait()

    rows = rows_ref[...].astype(F32)
    mean_sq = jnp.mean(rows * rows, axis=-1, keepdims=True)
    normed = (rows * lax.rsqrt(mean_sq + NORM_EPS) * norm_gain_ref[...]).astype(BF16)
    for j in range(n_tp):
        xb[j, ep] = normed[:, j * quarter : (j + 1) * quarter]
    meta[ep, :route_count] = ids_ref[...].astype(F32)
    meta[ep, route_count : 2 * route_count] = route_ref[...]

    pl.semaphore_wait(barrier, 1 + (nz - 1) + (n_tp - 1))

    near = jnp.minimum(z, nz - 1 - z)
    far_sign = jnp.where(z < nz - 1 - z, 1, -1)

    def origin(i):
        alternate = ((i + 1) // 2) * ((i % 2) * 2 - 1)
        return z + jnp.where(i <= 2 * near, alternate, far_sign * (i - near))

    def line_copy(buf, send, recv, zo, way):
        block = buf.at[zo * CORES + core]
        return remote(
            block,
            block,
            send.at[way, zo],
            recv.at[zo],
            (z + (1 if way == 0 else -1)) * CORES + core,
            tp,
        )

    def x_line(zo, h, way):
        block = xb.at[tp, zo * CORES + core, halves[h]]
        return remote(
            block,
            block,
            xs_s.at[way * 2 + h, zo],
            xs_r.at[h, zo],
            (z + (1 if way == 0 else -1)) * CORES + core,
            tp,
        )

    def each_x(zo, h, act_on):
        @pl.when((zo <= z) & (z < nz - 1))
        def _():
            act_on(x_line(zo, h, 0))

        @pl.when((zo >= z) & (z > 0))
        def _():
            act_on(x_line(zo, h, 1))

    def each_line(buf, send, recv, zo, act_on):
        @pl.when((zo <= z) & (z < nz - 1))
        def _():
            act_on(line_copy(buf, send, recv, zo, 0))

        @pl.when((zo >= z) & (z > 0))
        def _():
            act_on(line_copy(buf, send, recv, zo, 1))

    square = n_tp == 4
    half = tokens // 2
    side = tp + 1 - 2 * (tp % 2)
    other = (tp + 2) % n_tp
    across = (side + 2) % n_tp
    halves = (pl.ds(0, half), pl.ds(half, half))
    targets = [side, other] if square else [(tp + off) % n_tp for off in range(1, n_tp)]

    def tp_copy(zo, n, h):
        block = xb.at[tp, zo * CORES + core, halves[h]]
        return remote(block, block, t_s.at[h, n, zo], t_r.at[h, n, zo], ep, targets[n])

    def tp_arrival(zo, n, h):
        j = targets[n]
        block = xb.at[j, zo * CORES + core, halves[h]]
        k = n if square else len(targets) - 1 - n
        return remote(block, block, t_s.at[h, n, zo], t_r.at[h, k, zo], ep, j)

    def pass_copy(zo, n):
        block = xb.at[other if n == 0 else side, zo * CORES + core, halves[n]]
        return remote(block, block, h_s.at[n, zo], h_r.at[n, zo], ep, targets[n])

    def pass_arrival(zo, n):
        block = xb.at[across, zo * CORES + core, halves[n]]
        return remote(block, block, h_s.at[n, zo], h_r.at[n, zo], ep, targets[n])

    def pair_copy(j, zo, mine=True):
        block = xb.at[j, zo * CORES + (core if mine else 1 - core)]
        return remote(block, block, d_s.at[j, zo], d_r.at[j, zo], partner, tp)

    def pair_block(buf, send, recv, zo, mine=True):
        block = buf.at[zo * CORES + (core if mine else 1 - core)]
        return remote(block, block, send.at[zo], recv.at[zo], partner, tp)

    start = lambda copy: copy.start()

    def take_x(zo, h):
        x_line(zo, h, 0).wait_recv()
        each_x(zo, h, start)
        for n in range(len(targets)):
            tp_copy(zo, n, h).start()
        if h == 1:
            pair_copy(tp, zo).start()
            line_copy(meta, ms_s, ms_r, zo, 0).wait_recv()
            each_line(meta, ms_s, ms_r, zo, start)
            pair_block(meta, md_s, md_r, zo).start()

    def take_round(r, h):
        @pl.when(z + r < nz)
        def _():
            take_x(z + r, h)

        @pl.when(z - r >= 0)
        def _():
            take_x(z - r, h)

    def take_tp(zo, h):
        for n in range(len(targets)):
            tp_arrival(zo, n, h).wait_recv()
        if square:
            pass_copy(zo, h).start()
        if h == 1:
            for j in targets:
                pair_copy(j, zo).start()

    def take_pass(zo):
        if square:
            for n in range(2):
                pass_arrival(zo, n).wait_recv()
            pair_copy(across, zo).start()

    def take_pair(zo):
        for j in range(n_tp):
            pair_copy(j, zo, False).wait_recv()
        pair_block(meta, md_s, md_r, zo, False).wait_recv()

    def spread_kv(zo):
        each_line(kvb, ks_s, ks_r, zo, start)
        pair_block(kvb, kd_s, kd_r, zo).start()

    def take_kv(zo):
        line_copy(kvb, ks_s, ks_r, zo, 0).wait_recv()
        spread_kv(zo)

    def head_copy(zo):
        return remote(
            own.at[zo], kvb.at[ep], ks_s.at[0, zo], ks_r.at[z], zo * CORES + core, tp
        )

    def head_arrival(zo):
        block = kvb.at[zo * CORES + core]
        return remote(block, block, ks_s.at[0, zo], ks_r.at[zo], zo * CORES + core, tp)

    def head_pair(zo, mine=True):
        block = kvb.at[zo * CORES + (core if mine else 1 - core), pl.ds(1, 2)]
        return remote(block, block, kd_s.at[zo], kd_r.at[zo], partner, tp)

    def back_copy(zo):
        return remote(
            hsend.at[zo], hrecv.at[z], e_s.at[zo], e_r.at[z], zo * CORES + core, tp
        )

    def back_arrival(zo):
        return remote(
            hsend.at[zo], hrecv.at[zo], e_s.at[zo], e_r.at[zo], zo * CORES + core, tp
        )

    order = [across, side, other, tp] if square else [(tp + off) % n_tp for off in range(1, n_tp + 1)]

    def half_copy(zo, j):
        return remote(
            cbuf.at[zo, 1 - core, j], pbuf.at[zo, j], p_s.at[j, zo], p_r.at[j, zo], partner, tp
        )

    def term_parts():
        everything = pl.ds(0, tokens)
        if square:
            return [
                (side, halves[0], side, side),
                (across, halves[0], side, across),
                (other, halves[1], other, other),
                (across, halves[1], other, across),
                (other, halves[0], other, side),
                (side, halves[1], side, other),
            ]
        return [(j, everything, j, tp) for j in targets]

    def term_copy(zo, n):
        j, rows_of, device, slot = term_parts()[n]
        return remote(
            cbuf.at[zo, core, j, rows_of],
            rbuf.at[zo, slot, rows_of],
            r_s.at[n, zo],
            r_r.at[n, zo] if square else r_r.at[tp, zo],
            ep,
            device,
        )

    def term_arrival(zo, n):
        if square:
            slot = [tp, other, tp, side, across, across][n]
            rows_of = term_parts()[n][1]
            device = term_parts()[n][2]
            sem = r_r.at[n, zo]
        else:
            slot = device = targets[n]
            rows_of = pl.ds(0, tokens)
            sem = r_r.at[slot, zo]
        return remote(
            cbuf.at[zo, core, device, rows_of],
            rbuf.at[zo, slot, rows_of],
            r_s.at[n, zo],
            sem,
            ep,
            device,
        )

    def finish(zo):
        sends = {0: (1, 3), 1: (0,), 2: (2,)} if square else {i: (i,) for i in range(n_tp - 1)}
        for i, j in enumerate(order):
            half_copy(zo, j).wait_recv()
            cbuf[zo, core, j] = (
                cbuf[zo, core, j].astype(F32) + pbuf[zo, j].astype(F32)
            ).astype(BF16)
            for n in sends.get(i, ()):
                term_copy(zo, n).start()

    def middle(zo):
        if square:
            for n, arrived, j in ((4, 1, other), (5, 3, side)):
                term_arrival(zo, arrived).wait_recv()
                rows_of = halves[n - 4]
                cbuf[zo, core, j, rows_of] = (
                    cbuf[zo, core, j, rows_of].astype(F32) + rbuf[zo, j, rows_of].astype(F32)
                ).astype(BF16)
                term_copy(zo, n).start()

    def home_copy(zo):
        return remote(
            ubuf.at[zo], vbuf.at[z], v_s.at[zo], v_r.at[z], zo * CORES + core, tp
        )

    def home_arrival(zo):
        return remote(
            ubuf.at[zo], vbuf.at[zo], v_s.at[zo], v_r.at[zo], zo * CORES + core, tp
        )

    def reduce(zo):
        total = cbuf[zo, core, tp].astype(F32)
        if square:
            for n in (0, 2, 4, 5):
                term_arrival(zo, n).wait_recv()
            total = total + rbuf[zo, tp].astype(F32) + rbuf[zo, across].astype(F32)
        else:
            for n, j in enumerate(targets):
                term_arrival(zo, n).wait_recv()
                total = total + rbuf[zo, j].astype(F32)
        ubuf[zo] = total.astype(BF16)

        @pl.when(zo != z)
        def _():
            home_copy(zo).start()

    tile = min(256, hidden)
    tiles = hidden // tile

    def hidden_tile(zo, f):
        pair = pl.ds(zo * CORES, CORES)
        cols = pl.ds(f * tile, tile)
        gate = jnp.zeros((CORES * tokens, tile), F32)
        up = jnp.zeros((CORES * tokens, tile), F32)
        for j in range(n_tp):
            chunk = xb[j, pair].reshape(CORES * tokens, quarter)
            depth = pl.ds(j * quarter, quarter)
            gate = gate + jnp.dot(chunk, wg[depth, cols], preferred_element_type=F32)
            up = up + jnp.dot(chunk, wu[depth, cols], preferred_element_type=F32)
        gated = jnp.minimum(gate, CLAMP_LIMIT)
        clipped = jnp.clip(up, -CLAMP_LIMIT, CLAMP_LIMIT)
        act[:, cols] = (
            (clipped + 1.0) * gated * jax.nn.sigmoid(GATE_SLOPE * gated)
        ).astype(BF16)

    eye = lax.broadcasted_iota(jnp.int32, (tokens, tokens), 0) == lax.broadcasted_iota(
        jnp.int32, (tokens, tokens), 1
    )

    def route_scale(zo):
        columns = []
        for c in range(CORES):
            info = meta[zo * CORES + c]
            named = info[:route_count] == ep.astype(F32)
            weights = jnp.where(named, info[route_count : 2 * route_count], 0.0)
            line = jnp.sum(weights, axis=0, keepdims=True)
            columns.append(jnp.sum(jnp.where(eye, line, 0.0), axis=1, keepdims=True))
        return jnp.concatenate(columns, axis=0)

    def model_tiles(zo, places, scale):
        for j in places:
            cols = pl.ds(pl.multiple_of(j * quarter, quarter), quarter)
            value = jnp.dot(act[...], wd[:, cols], preferred_element_type=F32) * scale
            value = value.astype(BF16)
            for c in range(CORES):
                cbuf[zo, c, j] = value[c * tokens : (c + 1) * tokens]
        for j in places:
            half_copy(zo, j).start()

    for h in range(2):
        each_x(z, h, start)
    for j in range(n_tp):
        pair_copy(j, z).start()
    each_line(meta, ms_s, ms_r, z, start)
    pair_block(meta, md_s, md_r, z).start()

    tiles_early = tiles // 2
    early = len(order) // 2

    def split_heads():
        for copy in input_copies[4:]:
            copy.wait()
        for part, ref in enumerate((q_ref, k_ref, v_ref)):
            split[...] = ref[...].astype(F32)
            for h in range(heads):
                own[h, part] = split[pl.ds(h, tokens, stride=heads), :].astype(BF16)
        if by_head:
            kvb[ep] = own[z]
            head_pair(z).start()
        else:
            for h in range(heads):
                for part in range(2):
                    at = (part * heads + h) * width
                    kvb[ep, :, at : at + width] = own[h, 1 + part]

    def in_early(f):
        if f == 0:
            take_round(1, 0)
        if f == tiles - 2:
            take_round(1, 1)

    take_pair(z)
    for copy in weight_copies[:2]:
        copy.wait()
    for f in range(tiles):
        hidden_tile(z, f)
        in_early(f)
    weight_copies[2].wait()
    scale = route_scale(z)
    model_tiles(z, order[:early], scale)
    take_round(2, 0)
    take_tp(origin(1), 0)
    model_tiles(z, order[early:], scale)
    take_round(2, 1)
    take_tp(origin(1), 1)
    take_round(3, 0)
    if nz > 2:
        take_tp(origin(2), 0)
    split_heads()
    take_round(3, 1)
    if nz > 2:
        take_tp(origin(2), 1)
    if by_head:
        for off in range(1, nz):
            head_copy((z + off) % nz).start()
    else:
        spread_kv(z)
    take_pass(origin(1))

    gain = gain_ref[...]
    lane = lax.broadcasted_iota(jnp.int32, (tokens, width), 1)

    def both_maps(query):
        nothing = jnp.zeros_like(query)
        return jnp.concatenate(
            [jnp.where(lane < head_width, query, nothing), jnp.where(lane < head_width, nothing, query)],
            axis=0,
        )

    def lam_of(h):
        place = lax.broadcasted_iota(jnp.int32, lam_ref.shape, 1)
        return jnp.sum(jnp.where(place == h, lam_ref[...], 0.0), axis=1, keepdims=True)

    def head_norm(value_sum, total, lam):
        mean = value_sum / total
        attended = mean[:tokens] - lam * mean[tokens:]
        mean_sq = jnp.mean(attended * attended, axis=-1, keepdims=True)
        return (attended * lax.rsqrt(mean_sq + NORM_EPS) * gain).astype(BF16)

    def position_block(n):
        at = n * CORES + core
        extent = (n + 1) * CORES * tokens
        keys = kvb[: (n + 1) * CORES, 1].reshape(extent, width)
        values = kvb[: (n + 1) * CORES, 2].reshape(extent, width)
        score = lax.dot_general(
            both_maps(kvb[at, 0]), keys, (((1,), (1,)), ((), ())), preferred_element_type=F32
        ) * (head_width**-0.5)
        row = lax.broadcasted_iota(jnp.int32, (2 * tokens, extent), 0) % tokens + at * tokens
        col = lax.broadcasted_iota(jnp.int32, (2 * tokens, extent), 1)
        score = jnp.where(col <= row, score, -1e30)
        terms = jnp.exp(score - jnp.max(score, axis=1, keepdims=True))
        total = jnp.sum(terms, axis=1, keepdims=True)
        value_sum = jnp.dot(terms.astype(BF16), values, preferred_element_type=F32)
        result = head_norm(value_sum, total, lam_of(z))
        hsend[n] = result

        @pl.when(z != n)
        def _():
            back_copy(n).start()

    key_blocks = min(n_ep, 8)
    key_span = key_blocks * tokens

    def one_head(h, carry):
        both = both_maps(own[h, 0])
        row = lax.broadcasted_iota(jnp.int32, (2 * tokens, key_span), 0) % tokens + ep * tokens
        col = lax.broadcasted_iota(jnp.int32, (2 * tokens, key_span), 1)
        cols = pl.ds(pl.multiple_of(h * width, width), width)
        value_cols = pl.ds(pl.multiple_of((heads + h) * width, width), width)

        def span(s, state):
            top, total, value_sum = state
            blocks = pl.ds(s * key_blocks, key_blocks)
            keys = kvb[blocks, :, cols].reshape(key_span, width)
            values = kvb[blocks, :, value_cols].reshape(key_span, width)
            score = lax.dot_general(
                both, keys, (((1,), (1,)), ((), ())), preferred_element_type=F32
            ) * (head_width**-0.5)
            score = jnp.where(col + s * key_span <= row, score, -1e30)
            new_top = jnp.maximum(top, jnp.max(score, axis=1, keepdims=True))
            terms = jnp.exp(score - new_top)
            keep = jnp.exp(top - new_top)
            total = total * keep + jnp.sum(terms, axis=1, keepdims=True)
            value_sum = value_sum * keep + jnp.dot(
                terms.astype(BF16), values, preferred_element_type=F32
            )
            return new_top, total, value_sum

        state = (
            jnp.full((2 * tokens, 1), -1e30, F32),
            jnp.zeros((2 * tokens, 1), F32),
            jnp.zeros((2 * tokens, width), F32),
        )
        state = lax.fori_loop(0, n_ep // key_blocks, span, state)
        hsend[h] = head_norm(state[2], state[1], lam_of(h))
        return carry

    def take_heads():
        for off in range(1, nz):
            zs = (z + off) % nz
            head_arrival(zs).wait_recv()
            head_pair(zs).start()

    def step(i, carry):
        zo = origin(i)
        take_pair(zo)
        for f in range(tiles_early):
            hidden_tile(zo, f)

        take_round(i + 3, 0)
        take_round(i + 3, 1)

        @pl.when(i + 2 < nz)
        def _():
            take_tp(origin(i + 2), 0)

        @pl.when(i > 1)
        def _():
            finish(origin(i - 1))

        for f in range(tiles_early, tiles):
            hidden_tile(zo, f)

        @pl.when(i + 2 < nz)
        def _():
            take_tp(origin(i + 2), 1)

        @pl.when(i == 1)
        def _():
            finish(z)

        @pl.when(i + 1 < nz)
        def _():
            take_pass(origin(i + 1))

        @pl.when(i > 1)
        def _():
            middle(origin(i - 2))

        if by_head:

            @pl.when(i == nz - 2)
            def _():
                take_heads()

        scale = route_scale(zo)
        model_tiles(zo, order[:early], scale)

        @pl.when(i > 2)
        def _():
            reduce(origin(i - 3))

        model_tiles(zo, order[early:], scale)

        if not by_head:
            take_kv(zo)
        return carry

    lax.fori_loop(1, nz, step, 0)

    middle(origin(nz - 2))
    finish(origin(nz - 1))
    if by_head:
        for n in range(nz):
            head_pair(n, False).wait_recv()
        for n in range(nz):
            position_block(n)
        hrecv[z] = hsend[z]
        middle(origin(nz - 1))
        reduce(origin(nz - 3))
        reduce(origin(nz - 2))
        for off in range(1, nz):
            back_arrival((z + off) % nz).wait_recv()
        gathered = hrecv
    else:

        def wait_kv(i, carry):
            pair_block(kvb, kd_s, kd_r, i, False).wait_recv()
            return carry

        lax.fori_loop(0, nz, wait_kv, 0)
        lax.fori_loop(0, heads, one_head, 0)
        reduce(origin(nz - 3))
        middle(origin(nz - 1))
        reduce(origin(nz - 2))
        gathered = hsend
    head_rows = jnp.concatenate([gathered[h] for h in range(heads)], axis=1)
    weight_copies[3].wait()
    out_rows = tokens // n_tp

    for n in range(n_tp):
        cols = pl.ds(n * quarter, quarter)
        value = jnp.dot(head_rows, ow[:, cols], preferred_element_type=F32).astype(BF16)
        for j in range(n_tp):
            prod[j, :, cols] = value[j * out_rows : (j + 1) * out_rows]

    def row_copy(off):
        j = (tp + off) % n_tp
        return remote(prod.at[j], abuf.at[tp], a_s.at[off], a_r.at[tp], ep, j)

    def row_arrival(off):
        j = (tp + off) % n_tp
        return remote(prod.at[j], abuf.at[j], a_s.at[off], a_r.at[j], ep, j)

    reduce(origin(nz - 1))
    for off in range(1, n_tp):
        row_copy(off).start()

    mixed = prod[tp].astype(F32)
    for off in range(1, n_tp):
        row_arrival(off).wait_recv()
        mixed = mixed + abuf[(tp + off) % n_tp].astype(F32)
    out_rows_ref[...] = mixed

    combined = ubuf[z].astype(F32)
    for off in range(1, nz):
        zs = (z + off) % nz
        home_arrival(zs).wait_recv()
        combined = combined + vbuf[zs].astype(F32)
    out_exp_ref[...] = combined

    left = lambda copy: copy.wait_send()

    def drain(zo, carry):
        for h in range(2):
            each_x(zo, h, left)
        each_line(meta, ms_s, ms_r, zo, left)
        for n in range(len(term_parts())):
            term_copy(zo, n).wait_send()
        for j in range(n_tp):
            pair_copy(j, zo).wait_send()
            half_copy(zo, j).wait_send()
        pair_block(meta, md_s, md_r, zo).wait_send()
        if by_head:
            head_pair(zo).wait_send()
        else:
            each_line(kvb, ks_s, ks_r, zo, left)
            pair_block(kvb, kd_s, kd_r, zo).wait_send()

        @pl.when(zo != z)
        def _():
            home_copy(zo).wait_send()
            for n in range(len(targets)):
                for h in range(2):
                    tp_copy(zo, n, h).wait_send()
            if square:
                for n in range(2):
                    pass_copy(zo, n).wait_send()
            if by_head:
                head_copy(zo).wait_send()
                back_copy(zo).wait_send()

        return carry

    lax.fori_loop(0, nz, drain, 0)
    for off in range(1, n_tp):
        row_copy(off).wait_send()


def settle(rows_ref, exp_ref, out_rows_ref, out_exp_ref):
    out_rows_ref[...] = rows_ref[...].astype(BF16)
    out_exp_ref[...] = exp_ref[...].astype(BF16)


def body(
    query_maps,
    key_maps,
    value_rows,
    head_lambda,
    head_gain,
    out_weight,
    token_rows,
    norm_gain,
    expert_ids,
    route_weights,
    gate_weight,
    up_weight,
    down_weight,
):
    n_ep, n_tp = lax.axis_size("ep"), lax.axis_size("tp")
    nz = n_ep // CORES
    tokens, heads, width = query_maps.shape
    model = token_rows.shape[1]
    quarter = model // n_tp
    hidden = gate_weight.shape[2]
    routes = expert_ids.shape[1]
    span = heads * width
    by_head = heads == nz
    flat = (tokens * heads, width)
    vmem = pl.BlockSpec(memory_space=pltpu.VMEM)
    hbm = pl.BlockSpec(memory_space=pltpu.HBM)
    dma = pltpu.SemaphoreType.DMA
    line = [dma((2, nz)), dma((nz,))]
    line_sem = [dma((2, nz)), dma((2, nz))]
    len_targets = 2 if n_tp == 4 else n_tp - 1
    grid_sem = [dma((n_tp, nz)), dma((n_tp, nz))]
    pair = [dma((nz,)), dma((nz,))]
    mixed_rows, mixed_experts = pl.pallas_call(
        functools.partial(kernel, n_ep, n_tp, routes, width // 2, by_head),
        out_shape=(
            jax.ShapeDtypeStruct((tokens // n_tp, model), F32),
            jax.ShapeDtypeStruct((tokens, quarter), F32),
        ),
        in_specs=[hbm] * 13,
        out_specs=(vmem, vmem),
        scratch_shapes=[
            pltpu.VMEM(flat, BF16),
            pltpu.VMEM(flat, BF16),
            pltpu.VMEM(flat, BF16),
            pltpu.VMEM((1, heads), F32),
            pltpu.VMEM((1, width), F32),
            pltpu.VMEM((tokens, model), BF16),
            pltpu.VMEM((1, model), F32),
            pltpu.VMEM((routes, tokens), jnp.int32),
            pltpu.VMEM((routes, tokens), F32),
            pltpu.VMEM(out_weight.shape, BF16),
            pltpu.VMEM((model, hidden), BF16),
            pltpu.VMEM((model, hidden), BF16),
            pltpu.VMEM((hidden, model), BF16),
            pltpu.VMEM((n_tp, n_ep, tokens, quarter), BF16),
            pltpu.VMEM((n_ep, 2 * routes, tokens), F32),
            pltpu.VMEM((heads, 3, tokens, width), BF16),
            pltpu.VMEM((n_ep, 3, tokens, width) if by_head else (n_ep, tokens, 2 * span), BF16),
            pltpu.VMEM((heads, tokens, width), BF16),
            pltpu.VMEM((heads, tokens, width), BF16),
            pltpu.VMEM(flat, F32),
            pltpu.VMEM((CORES * tokens, hidden), BF16),
            pltpu.VMEM((nz, CORES, n_tp, tokens, quarter), BF16),
            pltpu.VMEM((nz, n_tp, tokens, quarter), BF16),
            pltpu.VMEM((nz, n_tp, tokens, quarter), BF16),
            pltpu.VMEM((nz, tokens, quarter), BF16),
            pltpu.VMEM((nz, tokens, quarter), BF16),
            pltpu.VMEM((n_tp, tokens // n_tp, model), BF16),
            pltpu.VMEM((n_tp, tokens // n_tp, model), BF16),
            dma((4, nz)),
            dma((2, nz)),
            *line,
            *line,
            dma((2, len_targets, nz)),
            dma((2, len_targets, nz)),
            *line_sem,
            *grid_sem,
            *pair,
            *pair,
            *grid_sem,
            dma((6 if n_tp == 4 else n_tp, nz)),
            dma((6 if n_tp == 4 else n_tp, nz)),
            *pair,
            *pair,
            dma((n_tp,)),
            dma((n_tp,)),
            dma((9,)),
            dma((4,)),
        ],
        compiler_params=pltpu.CompilerParams(
            collective_id=0, has_side_effects=True, vmem_limit_bytes=67043328
        ),
        name="layer",
    )(
        query_maps.reshape(flat),
        key_maps.reshape(flat),
        value_rows.reshape(flat),
        head_lambda.reshape(1, -1),
        head_gain.reshape(1, -1),
        token_rows,
        norm_gain.reshape(1, -1),
        expert_ids.T,
        route_weights.T,
        out_weight,
        gate_weight[0],
        up_weight[0],
        down_weight[0],
    )
    return pl.pallas_call(
        settle,
        out_shape=(
            jax.ShapeDtypeStruct(mixed_rows.shape, BF16),
            jax.ShapeDtypeStruct(mixed_experts.shape, BF16),
        ),
        in_specs=[vmem, vmem],
        out_specs=(vmem, vmem),
        name="settle",
    )(mixed_rows, mixed_experts)


def solution(mesh):
    placed = (
        P("ep", "tp", None),
        P("ep", "tp", None),
        P("ep", "tp", None),
        P("tp"),
        P(),
        P("tp", None),
        P("ep", None),
        P(),
        P("ep", None),
        P("ep", None),
        P("ep", None, "tp"),
        P("ep", None, "tp"),
        P("ep", "tp", None),
    )
    return jax.shard_map(
        body,
        mesh=mesh,
        in_specs=placed,
        out_specs=(P(("ep", "tp"), None), P("ep", "tp")),
        check_vma=False,
    )
```

```python
import functools

import jax
import jax.numpy as jnp
from jax import lax
from jax.experimental import pallas as pl
from jax.experimental.pallas import tpu as pltpu
from jax.sharding import PartitionSpec as P

NORM_EPS = 1e-05
CLAMP_LIMIT = 7.0
GATE_SLOPE = 1.702
CORES = 2
F32 = jnp.float32
BF16 = jnp.bfloat16


def remote(src, dst, send_sem, recv_sem, ep, tp):
    return pltpu.make_async_remote_copy(
        src_ref=src,
        dst_ref=dst,
        send_sem=send_sem,
        recv_sem=recv_sem,
        device_id={"ep": ep, "tp": tp},
        device_id_type=pl.DeviceIdType.MESH,
    )


def kernel(
    n_ep,
    n_tp,
    route_count,
    head_width,
    by_head,
    q_hbm,
    k_hbm,
    v_hbm,
    lam_hbm,
    gain_hbm,
    rows_hbm,
    norm_gain_hbm,
    ids_hbm,
    route_hbm,
    ow_hbm,
    wg_hbm,
    wu_hbm,
    wd_hbm,
    out_rows_ref,
    out_exp_ref,
    q_ref,
    k_ref,
    v_ref,
    lam_ref,
    gain_ref,
    rows_ref,
    norm_gain_ref,
    ids_ref,
    route_ref,
    ow,
    wg,
    wu,
    wd,
    xb,
    meta,
    own,
    kvb,
    hsend,
    hrecv,
    split,
    act,
    cbuf,
    pbuf,
    rbuf,
    ubuf,
    vbuf,
    prod,
    abuf,
    xs_s,
    xs_r,
    ms_s,
    ms_r,
    ks_s,
    ks_r,
    t_s,
    t_r,
    h_s,
    h_r,
    d_s,
    d_r,
    md_s,
    md_r,
    kd_s,
    kd_r,
    p_s,
    p_r,
    r_s,
    r_r,
    v_s,
    v_r,
    e_s,
    e_r,
    a_s,
    a_r,
    i_sem,
    w_sem,
):
    nz = n_ep // CORES
    ep = lax.axis_index("ep")
    tp = lax.axis_index("tp")
    z = ep // CORES
    core = ep % CORES
    partner = z * CORES + (1 - core)
    tokens, model = rows_ref.shape
    quarter = model // n_tp
    hidden = wg.shape[1]
    width = 2 * head_width
    heads = q_ref.shape[0] // tokens

    barrier = pltpu.get_barrier_semaphore()

    def greet(e, t):
        pl.semaphore_signal(
            barrier, inc=1, device_id={"ep": e, "tp": t}, device_id_type=pl.DeviceIdType.MESH
        )

    greet(partner, tp)
    for off in range(1, nz):
        greet(((z + off) % nz) * CORES + core, tp)
    for off in range(1, n_tp):
        greet(ep, (tp + off) % n_tp)

    inputs = [
        (rows_hbm, rows_ref),
        (norm_gain_hbm, norm_gain_ref),
        (ids_hbm, ids_ref),
        (route_hbm, route_ref),
        (q_hbm, q_ref),
        (k_hbm, k_ref),
        (v_hbm, v_ref),
        (lam_hbm, lam_ref),
        (gain_hbm, gain_ref),
    ]
    input_copies = [
        pltpu.make_async_copy(src, dst, i_sem.at[i]) for i, (src, dst) in enumerate(inputs)
    ]
    weight_copies = [
        pltpu.make_async_copy(src, dst, w_sem.at[i])
        for i, (src, dst) in enumerate([(wg_hbm, wg), (wu_hbm, wu), (wd_hbm, wd), (ow_hbm, ow)])
    ]
    for copy in input_copies + weight_copies:
        copy.start()
    for copy in input_copies[:4]:
        copy.wait()

    rows = rows_ref[...].astype(F32)
    mean_sq = jnp.mean(rows * rows, axis=-1, keepdims=True)
    normed = (rows * lax.rsqrt(mean_sq + NORM_EPS) * norm_gain_ref[...]).astype(BF16)
    for j in range(n_tp):
        xb[j, ep] = normed[:, j * quarter : (j + 1) * quarter]
    meta[ep, :route_count] = ids_ref[...].astype(F32)
    meta[ep, route_count : 2 * route_count] = route_ref[...]

    pl.semaphore_wait(barrier, 1 + (nz - 1) + (n_tp - 1))

    near = jnp.minimum(z, nz - 1 - z)
    far_sign = jnp.where(z < nz - 1 - z, 1, -1)

    def origin(i):
        alternate = ((i + 1) // 2) * ((i % 2) * 2 - 1)
        return z + jnp.where(i <= 2 * near, alternate, far_sign * (i - near))

    def line_copy(buf, send, recv, zo, way):
        block = buf.at[zo * CORES + core]
        return remote(
            block,
            block,
            send.at[way, zo],
            recv.at[zo],
            (z + (1 if way == 0 else -1)) * CORES + core,
            tp,
        )

    def x_line(zo, h, way):
        block = xb.at[tp, zo * CORES + core, halves[h]]
        return remote(
            block,
            block,
            xs_s.at[way * 2 + h, zo],
            xs_r.at[h, zo],
            (z + (1 if way == 0 else -1)) * CORES + core,
            tp,
        )

    def each_x(zo, h, act_on):
        @pl.when((zo <= z) & (z < nz - 1))
        def _():
            act_on(x_line(zo, h, 0))

        @pl.when((zo >= z) & (z > 0))
        def _():
            act_on(x_line(zo, h, 1))

    def each_line(buf, send, recv, zo, act_on):
        @pl.when((zo <= z) & (z < nz - 1))
        def _():
            act_on(line_copy(buf, send, recv, zo, 0))

        @pl.when((zo >= z) & (z > 0))
        def _():
            act_on(line_copy(buf, send, recv, zo, 1))

    square = n_tp == 4
    half = tokens // 2
    side = tp + 1 - 2 * (tp % 2)
    other = (tp + 2) % n_tp
    across = (side + 2) % n_tp
    halves = (pl.ds(0, half), pl.ds(half, half))
    targets = [side, other] if square else [(tp + off) % n_tp for off in range(1, n_tp)]

    def tp_copy(zo, n, h):
        block = xb.at[tp, zo * CORES + core, halves[h]]
        return remote(block, block, t_s.at[zo], t_r.at[h, n, zo], ep, targets[n])

    def tp_arrival(zo, n, h):
        j = targets[n]
        block = xb.at[j, zo * CORES + core, halves[h]]
        k = n if square else len(targets) - 1 - n
        return remote(block, block, t_s.at[zo], t_r.at[h, k, zo], ep, j)

    def pass_copy(zo, n):
        block = xb.at[other if n == 0 else side, zo * CORES + core, halves[n]]
        return remote(block, block, h_s.at[n, zo], h_r.at[n, zo], ep, targets[n])

    def pass_arrival(zo, n):
        block = xb.at[across, zo * CORES + core, halves[n]]
        return remote(block, block, h_s.at[n, zo], h_r.at[n, zo], ep, targets[n])

    def pair_copy(j, zo, mine=True):
        block = xb.at[j, zo * CORES + (core if mine else 1 - core)]
        return remote(block, block, d_s.at[zo], d_r.at[zo], partner, tp)

    def pair_all(zo, mine=True):
        block = xb.at[:, zo * CORES + (core if mine else 1 - core)]
        return remote(block, block, d_s.at[zo], d_r.at[zo], partner, tp)

    def pair_block(buf, send, recv, zo, mine=True):
        block = buf.at[zo * CORES + (core if mine else 1 - core)]
        return remote(block, block, send.at[zo], recv.at[zo], partner, tp)

    start = lambda copy: copy.start()

    def take_x(zo, h):
        x_line(zo, h, 0).wait_recv()
        each_x(zo, h, start)
        for n in range(len(targets)):
            tp_copy(zo, n, h).start()
        if h == 1:
            pair_copy(tp, zo).start()
            line_copy(meta, ms_s, ms_r, zo, 0).wait_recv()
            each_line(meta, ms_s, ms_r, zo, start)
            pair_block(meta, md_s, md_r, zo).start()

    def take_round(r, h):
        @pl.when(z + r < nz)
        def _():
            take_x(z + r, h)

        @pl.when(z - r >= 0)
        def _():
            take_x(z - r, h)

    def take_tp(zo, h):
        for n in range(len(targets)):
            tp_arrival(zo, n, h).wait_recv()
        if square:
            pass_copy(zo, h).start()
        if h == 1:
            for j in targets:
                pair_copy(j, zo).start()

    def take_pass(zo):
        if square:
            for n in range(2):
                pass_arrival(zo, n).wait_recv()
            pair_copy(across, zo).start()

    def take_pair(zo):
        pair_all(zo, False).wait_recv()
        pair_block(meta, md_s, md_r, zo, False).wait_recv()

    def spread_kv(zo):
        each_line(kvb, ks_s, ks_r, zo, start)
        pair_block(kvb, kd_s, kd_r, zo).start()

    def take_kv(zo):
        line_copy(kvb, ks_s, ks_r, zo, 0).wait_recv()
        spread_kv(zo)

    def head_copy(zo):
        return remote(
            own.at[zo], kvb.at[ep], ks_s.at[0, zo], ks_r.at[z], zo * CORES + core, tp
        )

    def head_arrival(zo):
        block = kvb.at[zo * CORES + core]
        return remote(block, block, ks_s.at[0, zo], ks_r.at[zo], zo * CORES + core, tp)

    def head_pair(zo, mine=True):
        block = kvb.at[zo * CORES + (core if mine else 1 - core), pl.ds(1, 2)]
        return remote(block, block, kd_s.at[zo], kd_r.at[zo], partner, tp)

    def back_copy(zo):
        return remote(
            hsend.at[zo], hrecv.at[z], e_s.at[zo], e_r.at[z], zo * CORES + core, tp
        )

    def back_arrival(zo):
        return remote(
            hsend.at[zo], hrecv.at[zo], e_s.at[zo], e_r.at[zo], zo * CORES + core, tp
        )

    order = [across, side, other, tp] if square else [(tp + off) % n_tp for off in range(1, n_tp + 1)]

    def half_copy(zo, j):
        return remote(
            cbuf.at[zo, 1 - core, j], pbuf.at[zo, j], p_s.at[zo], p_r.at[j, zo], partner, tp
        )

    def term_parts():
        everything = pl.ds(0, tokens)
        if square:
            return [
                (side, halves[0], side, side),
                (across, halves[0], side, across),
                (other, halves[1], other, other),
                (across, halves[1], other, across),
                (other, halves[0], other, side),
                (side, halves[1], side, other),
            ]
        return [(j, everything, j, tp) for j in targets]

    def term_copy(zo, n):
        j, rows_of, device, slot = term_parts()[n]
        return remote(
            cbuf.at[zo, core, j, rows_of],
            rbuf.at[zo, slot, rows_of],
            r_s.at[zo],
            r_r.at[n, zo] if square else r_r.at[tp, zo],
            ep,
            device,
        )

    def term_arrival(zo, n):
        if square:
            slot = [tp, other, tp, side, across, across][n]
            rows_of = term_parts()[n][1]
            device = term_parts()[n][2]
            sem = r_r.at[n, zo]
        else:
            slot = device = targets[n]
            rows_of = pl.ds(0, tokens)
            sem = r_r.at[slot, zo]
        return remote(
            cbuf.at[zo, core, device, rows_of],
            rbuf.at[zo, slot, rows_of],
            r_s.at[zo],
            sem,
            ep,
            device,
        )

    def finish(zo):
        sends = {0: (1, 3), 1: (0,), 2: (2,)} if square else {i: (i,) for i in range(n_tp - 1)}
        for i, j in enumerate(order):
            half_copy(zo, j).wait_recv()
            cbuf[zo, core, j] = (
                cbuf[zo, core, j].astype(F32) + pbuf[zo, j].astype(F32)
            ).astype(BF16)
            for n in sends.get(i, ()):
                term_copy(zo, n).start()

    def middle(zo):
        if square:
            for n, arrived, j in ((4, 1, other), (5, 3, side)):
                term_arrival(zo, arrived).wait_recv()
                rows_of = halves[n - 4]
                cbuf[zo, core, j, rows_of] = (
                    cbuf[zo, core, j, rows_of].astype(F32) + rbuf[zo, j, rows_of].astype(F32)
                ).astype(BF16)
                term_copy(zo, n).start()

    def home_copy(zo):
        return remote(
            ubuf.at[zo], vbuf.at[z], v_s.at[zo], v_r.at[z], zo * CORES + core, tp
        )

    def home_arrival(zo):
        return remote(
            ubuf.at[zo], vbuf.at[zo], v_s.at[zo], v_r.at[zo], zo * CORES + core, tp
        )

    def reduce(zo):
        total = cbuf[zo, core, tp].astype(F32)
        if square:
            for n in (0, 2, 4, 5):
                term_arrival(zo, n).wait_recv()
            total = total + rbuf[zo, tp].astype(F32) + rbuf[zo, across].astype(F32)
        else:
            for n, j in enumerate(targets):
                term_arrival(zo, n).wait_recv()
                total = total + rbuf[zo, j].astype(F32)
        ubuf[zo] = total.astype(BF16)

        @pl.when(zo != z)
        def _():
            home_copy(zo).start()

    tile = min(256, hidden)
    tiles = hidden // tile

    def hidden_tile(zo, f):
        pair = pl.ds(zo * CORES, CORES)
        cols = pl.ds(f * tile, tile)
        gate = jnp.zeros((CORES * tokens, tile), F32)
        up = jnp.zeros((CORES * tokens, tile), F32)
        for j in range(n_tp):
            chunk = xb[j, pair].reshape(CORES * tokens, quarter)
            depth = pl.ds(j * quarter, quarter)
            gate = gate + jnp.dot(chunk, wg[depth, cols], preferred_element_type=F32)
            up = up + jnp.dot(chunk, wu[depth, cols], preferred_element_type=F32)
        gated = jnp.minimum(gate, CLAMP_LIMIT)
        clipped = jnp.clip(up, -CLAMP_LIMIT, CLAMP_LIMIT)
        act[:, cols] = (
            (clipped + 1.0) * gated * jax.nn.sigmoid(GATE_SLOPE * gated)
        ).astype(BF16)

    eye = lax.broadcasted_iota(jnp.int32, (tokens, tokens), 0) == lax.broadcasted_iota(
        jnp.int32, (tokens, tokens), 1
    )

    def route_scale(zo):
        columns = []
        for c in range(CORES):
            info = meta[zo * CORES + c]
            named = info[:route_count] == ep.astype(F32)
            weights = jnp.where(named, info[route_count : 2 * route_count], 0.0)
            line = jnp.sum(weights, axis=0, keepdims=True)
            columns.append(jnp.sum(jnp.where(eye, line, 0.0), axis=1, keepdims=True))
        return jnp.concatenate(columns, axis=0)

    def model_tiles(zo, places, scale):
        for j in places:
            cols = pl.ds(pl.multiple_of(j * quarter, quarter), quarter)
            value = jnp.dot(act[...], wd[:, cols], preferred_element_type=F32) * scale
            value = value.astype(BF16)
            for c in range(CORES):
                cbuf[zo, c, j] = value[c * tokens : (c + 1) * tokens]
        for j in places:
            half_copy(zo, j).start()

    for h in range(2):
        each_x(z, h, start)
    for j in range(n_tp):
        pair_copy(j, z).start()
    each_line(meta, ms_s, ms_r, z, start)
    pair_block(meta, md_s, md_r, z).start()

    tiles_early = tiles // 2
    early = len(order) // 2

    def split_heads():
        for copy in input_copies[4:]:
            copy.wait()
        for part, ref in enumerate((q_ref, k_ref, v_ref)):
            split[...] = ref[...].astype(F32)
            for h in range(heads):
                own[h, part] = split[pl.ds(h, tokens, stride=heads), :].astype(BF16)
        if by_head:
            kvb[ep] = own[z]
            head_pair(z).start()
        else:
            for h in range(heads):
                for part in range(2):
                    at = (part * heads + h) * width
                    kvb[ep, :, at : at + width] = own[h, 1 + part]

    def in_early(f):
        if f == 0:
            take_round(1, 0)
        if f == tiles - 2:
            take_round(1, 1)

    take_pair(z)
    for copy in weight_copies[:2]:
        copy.wait()
    for f in range(tiles):
        hidden_tile(z, f)
        in_early(f)
    weight_copies[2].wait()
    scale = route_scale(z)
    model_tiles(z, order[:early], scale)
    take_round(2, 0)
    take_tp(origin(1), 0)
    model_tiles(z, order[early:], scale)
    take_round(2, 1)
    take_tp(origin(1), 1)
    take_round(3, 0)
    if nz > 2:
        take_tp(origin(2), 0)
    split_heads()
    take_round(3, 1)
    if nz > 2:
        take_tp(origin(2), 1)
    if by_head:
        for off in range(1, nz):
            head_copy((z + off) % nz).start()
    else:
        spread_kv(z)
    take_pass(origin(1))

    gain = gain_ref[...]
    lane = lax.broadcasted_iota(jnp.int32, (tokens, width), 1)

    def both_maps(query):
        nothing = jnp.zeros_like(query)
        return jnp.concatenate(
            [jnp.where(lane < head_width, query, nothing), jnp.where(lane < head_width, nothing, query)],
            axis=0,
        )

    def lam_of(h):
        place = lax.broadcasted_iota(jnp.int32, lam_ref.shape, 1)
        return jnp.sum(jnp.where(place == h, lam_ref[...], 0.0), axis=1, keepdims=True)

    def head_norm(value_sum, total, lam):
        mean = value_sum / total
        attended = mean[:tokens] - lam * mean[tokens:]
        mean_sq = jnp.mean(attended * attended, axis=-1, keepdims=True)
        return (attended * lax.rsqrt(mean_sq + NORM_EPS) * gain).astype(BF16)

    def position_block(n):
        at = n * CORES + core
        extent = (n + 1) * CORES * tokens
        keys = kvb[: (n + 1) * CORES, 1].reshape(extent, width)
        values = kvb[: (n + 1) * CORES, 2].reshape(extent, width)
        score = lax.dot_general(
            both_maps(kvb[at, 0]), keys, (((1,), (1,)), ((), ())), preferred_element_type=F32
        ) * (head_width**-0.5)
        row = lax.broadcasted_iota(jnp.int32, (2 * tokens, extent), 0) % tokens + at * tokens
        col = lax.broadcasted_iota(jnp.int32, (2 * tokens, extent), 1)
        score = jnp.where(col <= row, score, -1e30)
        terms = jnp.exp(score - jnp.max(score, axis=1, keepdims=True))
        total = jnp.sum(terms, axis=1, keepdims=True)
        value_sum = jnp.dot(terms.astype(BF16), values, preferred_element_type=F32)
        result = head_norm(value_sum, total, lam_of(z))
        hsend[n] = result

        @pl.when(z != n)
        def _():
            back_copy(n).start()

    key_blocks = min(n_ep, 8)
    key_span = key_blocks * tokens

    def one_head(h, carry):
        both = both_maps(own[h, 0])
        row = lax.broadcasted_iota(jnp.int32, (2 * tokens, key_span), 0) % tokens + ep * tokens
        col = lax.broadcasted_iota(jnp.int32, (2 * tokens, key_span), 1)
        cols = pl.ds(pl.multiple_of(h * width, width), width)
        value_cols = pl.ds(pl.multiple_of((heads + h) * width, width), width)

        def span(s, state):
            top, total, value_sum = state
            blocks = pl.ds(s * key_blocks, key_blocks)
            keys = kvb[blocks, :, cols].reshape(key_span, width)
            values = kvb[blocks, :, value_cols].reshape(key_span, width)
            score = lax.dot_general(
                both, keys, (((1,), (1,)), ((), ())), preferred_element_type=F32
            ) * (head_width**-0.5)
            score = jnp.where(col + s * key_span <= row, score, -1e30)
            new_top = jnp.maximum(top, jnp.max(score, axis=1, keepdims=True))
            terms = jnp.exp(score - new_top)
            keep = jnp.exp(top - new_top)
            total = total * keep + jnp.sum(terms, axis=1, keepdims=True)
            value_sum = value_sum * keep + jnp.dot(
                terms.astype(BF16), values, preferred_element_type=F32
            )
            return new_top, total, value_sum

        state = (
            jnp.full((2 * tokens, 1), -1e30, F32),
            jnp.zeros((2 * tokens, 1), F32),
            jnp.zeros((2 * tokens, width), F32),
        )
        state = lax.fori_loop(0, n_ep // key_blocks, span, state)
        hsend[h] = head_norm(state[2], state[1], lam_of(h))
        return carry

    def take_heads():
        for off in range(1, nz):
            zs = (z + off) % nz
            head_arrival(zs).wait_recv()
            head_pair(zs).start()

    def step(i, carry):
        zo = origin(i)
        take_pair(zo)
        for f in range(tiles_early):
            hidden_tile(zo, f)

        take_round(i + 3, 0)
        take_round(i + 3, 1)

        @pl.when(i + 2 < nz)
        def _():
            take_tp(origin(i + 2), 0)

        finish(origin(i - 1))

        for f in range(tiles_early, tiles):
            hidden_tile(zo, f)

        @pl.when(i + 2 < nz)
        def _():
            take_tp(origin(i + 2), 1)

        @pl.when(i + 1 < nz)
        def _():
            take_pass(origin(i + 1))

        @pl.when(i > 1)
        def _():
            middle(origin(i - 2))

        if by_head:

            @pl.when(i == nz - 2)
            def _():
                take_heads()

        scale = route_scale(zo)
        model_tiles(zo, order[:early], scale)

        @pl.when(i > 2)
        def _():
            reduce(origin(i - 3))

        model_tiles(zo, order[early:], scale)

        if not by_head:
            take_kv(zo)
        return carry

    lax.fori_loop(1, nz, step, 0)

    middle(origin(nz - 2))
    finish(origin(nz - 1))
    if by_head:
        for n in range(nz):
            head_pair(n, False).wait_recv()
        for n in range(nz):
            position_block(n)
        hrecv[z] = hsend[z]
        reduce(origin(nz - 3))
        reduce(origin(nz - 2))
        middle(origin(nz - 1))
        for off in range(1, nz):
            back_arrival((z + off) % nz).wait_recv()
        gathered = hrecv
    else:

        def wait_kv(i, carry):
            pair_block(kvb, kd_s, kd_r, i, False).wait_recv()
            return carry

        lax.fori_loop(0, nz, wait_kv, 0)
        lax.fori_loop(0, heads, one_head, 0)
        reduce(origin(nz - 3))
        middle(origin(nz - 1))
        reduce(origin(nz - 2))
        gathered = hsend
    head_rows = jnp.concatenate([gathered[h] for h in range(heads)], axis=1)
    weight_copies[3].wait()
    out_rows = tokens // n_tp

    for n in range(n_tp):
        cols = pl.ds(n * quarter, quarter)
        value = jnp.dot(head_rows, ow[:, cols], preferred_element_type=F32).astype(BF16)
        for j in range(n_tp):
            prod[j, :, cols] = value[j * out_rows : (j + 1) * out_rows]

    def row_copy(off):
        j = (tp + off) % n_tp
        return remote(prod.at[j], abuf.at[tp], a_s.at[off], a_r.at[tp], ep, j)

    def row_arrival(off):
        j = (tp + off) % n_tp
        return remote(prod.at[j], abuf.at[j], a_s.at[off], a_r.at[j], ep, j)

    reduce(origin(nz - 1))
    for off in range(1, n_tp):
        row_copy(off).start()

    mixed = prod[tp].astype(F32)
    for off in range(1, n_tp):
        row_arrival(off).wait_recv()
        mixed = mixed + abuf[(tp + off) % n_tp].astype(F32)
    out_rows_ref[...] = mixed

    combined = ubuf[z].astype(F32)
    for off in range(1, nz):
        zs = (z + off) % nz
        home_arrival(zs).wait_recv()
        combined = combined + vbuf[zs].astype(F32)
    out_exp_ref[...] = combined

    left = lambda copy: copy.wait_send()

    def drain(zo, carry):
        for h in range(2):
            each_x(zo, h, left)
        each_line(meta, ms_s, ms_r, zo, left)
        terms = cbuf.at[zo, core, pl.ds(0, n_tp - 1)]
        remote(terms, terms, r_s.at[zo], r_r.at[0, zo], partner, tp).wait_send()
        pair_all(zo).wait_send()
        remote(
            cbuf.at[zo, 1 - core], pbuf.at[zo], p_s.at[zo], p_r.at[0, zo], partner, tp
        ).wait_send()
        pair_block(meta, md_s, md_r, zo).wait_send()
        if by_head:
            head_pair(zo).wait_send()
        else:
            each_line(kvb, ks_s, ks_r, zo, left)
            pair_block(kvb, kd_s, kd_r, zo).wait_send()

        @pl.when(zo != z)
        def _():
            home_copy(zo).wait_send()
            spread = xb.at[pl.ds(0, len(targets)), zo * CORES + core]
            remote(spread, spread, t_s.at[zo], t_r.at[0, 0, zo], partner, tp).wait_send()
            if square:
                for n in range(2):
                    pass_copy(zo, n).wait_send()
            if by_head:
                head_copy(zo).wait_send()
                back_copy(zo).wait_send()

        return carry

    lax.fori_loop(0, nz, drain, 0)
    for off in range(1, n_tp):
        row_copy(off).wait_send()


def settle(rows_ref, exp_ref, out_rows_ref, out_exp_ref):
    out_rows_ref[...] = rows_ref[...].astype(BF16)
    out_exp_ref[...] = exp_ref[...].astype(BF16)


def body(
    query_maps,
    key_maps,
    value_rows,
    head_lambda,
    head_gain,
    out_weight,
    token_rows,
    norm_gain,
    expert_ids,
    route_weights,
    gate_weight,
    up_weight,
    down_weight,
):
    n_ep, n_tp = lax.axis_size("ep"), lax.axis_size("tp")
    nz = n_ep // CORES
    tokens, heads, width = query_maps.shape
    model = token_rows.shape[1]
    quarter = model // n_tp
    hidden = gate_weight.shape[2]
    routes = expert_ids.shape[1]
    span = heads * width
    by_head = heads == nz
    flat = (tokens * heads, width)
    vmem = pl.BlockSpec(memory_space=pltpu.VMEM)
    hbm = pl.BlockSpec(memory_space=pltpu.HBM)
    dma = pltpu.SemaphoreType.DMA
    line = [dma((2, nz)), dma((nz,))]
    line_sem = [dma((2, nz)), dma((2, nz))]
    len_targets = 2 if n_tp == 4 else n_tp - 1
    pair = [dma((nz,)), dma((nz,))]
    mixed_rows, mixed_experts = pl.pallas_call(
        functools.partial(kernel, n_ep, n_tp, routes, width // 2, by_head),
        out_shape=(
            jax.ShapeDtypeStruct((tokens // n_tp, model), F32),
            jax.ShapeDtypeStruct((tokens, quarter), F32),
        ),
        in_specs=[hbm] * 13,
        out_specs=(vmem, vmem),
        scratch_shapes=[
            pltpu.VMEM(flat, BF16),
            pltpu.VMEM(flat, BF16),
            pltpu.VMEM(flat, BF16),
            pltpu.VMEM((1, heads), F32),
            pltpu.VMEM((1, width), F32),
            pltpu.VMEM((tokens, model), BF16),
            pltpu.VMEM((1, model), F32),
            pltpu.VMEM((routes, tokens), jnp.int32),
            pltpu.VMEM((routes, tokens), F32),
            pltpu.VMEM(out_weight.shape, BF16),
            pltpu.VMEM((model, hidden), BF16),
            pltpu.VMEM((model, hidden), BF16),
            pltpu.VMEM((hidden, model), BF16),
            pltpu.VMEM((n_tp, n_ep, tokens, quarter), BF16),
            pltpu.VMEM((n_ep, 2 * routes, tokens), F32),
            pltpu.VMEM((heads, 3, tokens, width), BF16),
            pltpu.VMEM((n_ep, 3, tokens, width) if by_head else (n_ep, tokens, 2 * span), BF16),
            pltpu.VMEM((heads, tokens, width), BF16),
            pltpu.VMEM((heads, tokens, width), BF16),
            pltpu.VMEM(flat, F32),
            pltpu.VMEM((CORES * tokens, hidden), BF16),
            pltpu.VMEM((nz, CORES, n_tp, tokens, quarter), BF16),
            pltpu.VMEM((nz, n_tp, tokens, quarter), BF16),
            pltpu.VMEM((nz, n_tp, tokens, quarter), BF16),
            pltpu.VMEM((nz, tokens, quarter), BF16),
            pltpu.VMEM((nz, tokens, quarter), BF16),
            pltpu.VMEM((n_tp, tokens // n_tp, model), BF16),
            pltpu.VMEM((n_tp, tokens // n_tp, model), BF16),
            dma((4, nz)),
            dma((2, nz)),
            *line,
            *line,
            dma((nz,)),
            dma((2, len_targets, nz)),
            *line_sem,
            *pair,
            *pair,
            *pair,
            dma((nz,)),
            dma((n_tp, nz)),
            dma((nz,)),
            dma((6 if n_tp == 4 else n_tp, nz)),
            *pair,
            *pair,
            dma((n_tp,)),
            dma((n_tp,)),
            dma((9,)),
            dma((4,)),
        ],
        compiler_params=pltpu.CompilerParams(
            collective_id=0, has_side_effects=True, vmem_limit_bytes=67043328
        ),
        name="layer",
    )(
        query_maps.reshape(flat),
        key_maps.reshape(flat),
        value_rows.reshape(flat),
        head_lambda.reshape(1, -1),
        head_gain.reshape(1, -1),
        token_rows,
        norm_gain.reshape(1, -1),
        expert_ids.T,
        route_weights.T,
        out_weight,
        gate_weight[0],
        up_weight[0],
        down_weight[0],
    )
    return pl.pallas_call(
        settle,
        out_shape=(
            jax.ShapeDtypeStruct(mixed_rows.shape, BF16),
            jax.ShapeDtypeStruct(mixed_experts.shape, BF16),
        ),
        in_specs=[vmem, vmem],
        out_specs=(vmem, vmem),
        name="settle",
    )(mixed_rows, mixed_experts)


def solution(mesh):
    placed = (
        P("ep", "tp", None),
        P("ep", "tp", None),
        P("ep", "tp", None),
        P("tp"),
        P(),
        P("tp", None),
        P("ep", None),
        P(),
        P("ep", None),
        P("ep", None),
        P("ep", None, "tp"),
        P("ep", None, "tp"),
        P("ep", "tp", None),
    )
    return jax.shard_map(
        body,
        mesh=mesh,
        in_specs=placed,
        out_specs=(P(("ep", "tp"), None), P("ep", "tp")),
        check_vma=False,
    )
```
